32 devices in a mesh: sp: 8 (over z, y), tp: 4 (over x, core).
Axes of the slice: x: 2, y: 2, z: 4, core: 2. Of those that a mesh axis runs over, the one named last changes fastest.
Arguments:
- queries: bfloat16 [4096, 1024], P('sp', 'tp'), may hold values from -200 to 200
- keys: bfloat16 [4096, 1024], P('sp', 'tp'), may hold values from -6 to 6
- values: bfloat16 [4096, 1024], P('sp', 'tp'), may hold values from -24 to 24
- cum_gate: float32 [4096, 8], P('sp', 'tp'), may hold values from -414 to 0, as said below
- residual: bfloat16 [4096, 2048], P(('sp', 'tp')), may hold values from -1.5 to 1.5
- w_out: bfloat16 [1024, 2048], replicated, may hold values from -0.1875 to 0.1875
- gain: float32 [2048], replicated, may hold values from 0.1 to 1.9
- w_up: bfloat16 [2048, 8192], P('sp', 'tp'), may hold values from -0.125 to 0.125
- w_down: bfloat16 [8192, 2048], P('tp', 'sp'), may hold values from -0.0625 to 0.0625
Outputs:
- output: bfloat16 [4096, 2048], P(('sp', 'tp'))
The draws below stay inside these ranges and needn't reach their ends.
Inputs may be any that keep to these rules, and one draw needn't show every extreme that they name: Within each head, cum_gate never rises from one position to the next.
All inputs are finite; a program needn't handle non-finite values.
Results may differ from the reference program's by a relative error of at most 0.022.
Values may be sent and summed in bfloat16 or wider, within the bound.
No kernel may reach another device: no remote copies, remote signals or barrier semaphores. Data moves between devices by JAX's collectives and lax.ppermute only.
A program may use at most 128 MiB of HBM per device.

```python
import math
import jax
import jax.numpy as jnp
from jax import lax

D = 2048
HEADS = 8
HEAD_DIM = 128
FF = 8192
TOK_DEV = 512
SEQUENCE_TOKENS = 4096
N_TP = 4


def joint_pair(key):
    width = HEADS * HEAD_DIM
    query_key = jax.random.fold_in(key, 101)
    key_key = jax.random.fold_in(key, 202)
    keys = jnp.clip(jax.random.normal(key_key, (SEQUENCE_TOKENS, width), jnp.float32), -6.0, 6.0)
    queries = jnp.clip(2.0 * jax.random.normal(query_key, (SEQUENCE_TOKENS, width), jnp.float32), -12.0, 12.0)
    return (queries, keys)


def draw_queries(key, part):
    return joint_pair(key)[0].astype(jnp.bfloat16)


def draw_keys(key, part):
    return joint_pair(key)[1].astype(jnp.bfloat16)


def draw_cum_gate(key, part):
    shuffle_random_key, gradual_decay_key, quick_decay_key, block_random_key, jitter_random_key, spike_random_key, layer_depth_key = jax.random.split(key, 7)
    order = jax.random.permutation(shuffle_random_key, HEADS)
    slow = order < HEADS // 2
    slow_rate = jax.random.uniform(gradual_decay_key, (HEADS,), jnp.float32, 0.2, 0.6) / SEQUENCE_TOKENS
    fast_rate = 1.0 / jnp.exp(jax.random.uniform(quick_decay_key, (HEADS,), jnp.float32, math.log(30.0), math.log(100.0)))
    rate = jnp.where(slow, slow_rate, fast_rate)
    shards = SEQUENCE_TOKENS // TOK_DEV
    factor = 2.0 ** jax.random.uniform(block_random_key, (shards, HEADS), jnp.float32, -1.0, 1.0)
    token_positions = jnp.arange(SEQUENCE_TOKENS)
    per_row = factor[token_positions // TOK_DEV]
    noise = jax.random.uniform(jitter_random_key, (SEQUENCE_TOKENS, HEADS), jnp.float32, 0.5, 1.5)
    steps = -rate[None, :] * per_row * noise
    spike_events = jax.random.randint(spike_random_key, (3,), 0, SEQUENCE_TOKENS)
    depth = jnp.log(jax.random.uniform(layer_depth_key, (3, HEADS), jnp.float32, 0.6, 0.8))
    match_events = (token_positions[:, None] == spike_events[None, :]).astype(jnp.float32)
    steps = steps + jnp.dot(match_events, depth) * slow.astype(jnp.float32)[None, :]
    return jnp.cumsum(steps, axis=0)


def level_of(own_key, extent, pieces, smallest, top_value):
    level, own = 1.0, jax.random.fold_in(own_key, 6)
    for axis_at, shards_of in pieces:
        heights = jnp.exp(jax.random.uniform(jax.random.fold_in(own, axis_at), (shards_of,), jnp.float32, smallest / len(pieces), top_value / len(pieces)))
        level = level * jnp.repeat(heights, extent[axis_at] // shards_of).reshape([-1 if axis == axis_at else 1 for axis in range(len(extent))])
    return level


def centred(rng, shape, scale, limit, pieces=(), held_as=jnp.bfloat16):
    drawn = jax.random.normal(rng, shape, jnp.float32) * scale
    if len(pieces) > 0:
        drawn = level_of(rng, shape, pieces, -0.22, 0.18) * drawn
    return jnp.clip(drawn, min=-limit, max=limit).astype(held_as)


def setup_inputs(seed: int = 0) -> dict:
    streams_of = jax.random.split(jax.random.key(seed), 10)
    queries = draw_queries(jax.random.fold_in(streams_of[9], 71), 0)
    keys = draw_keys(jax.random.fold_in(streams_of[9], 71), 0)
    values = centred(streams_of[2], (SEQUENCE_TOKENS, HEADS * HEAD_DIM), 4.0, 24.0, ((0, 8), (1, 4)))
    cum_gate = draw_cum_gate(jax.random.fold_in(streams_of[9], 71), 0)
    residual = centred(streams_of[4], (SEQUENCE_TOKENS, D), 0.25, 1.5, ((0, 32),))
    w_out = centred(streams_of[5], (HEADS * HEAD_DIM, D), (HEADS * HEAD_DIM) ** -0.5, 0.1875)
    gain = jnp.clip(1.0 + 0.18 * jax.random.normal(streams_of[6], (D,), jnp.float32), 0.1, 1.9)
    w_up = centred(streams_of[7], (D, FF), D ** -0.5, 0.125, ((0, 8), (1, 4)))
    w_down = centred(streams_of[8], (FF, D), FF ** -0.5, 0.0625, ((0, 4), (1, 8)))
    return dict(queries=queries, keys=keys, values=values, cum_gate=cum_gate, residual=residual, w_out=w_out, gain=gain, w_up=w_up, w_down=w_down)


def reference(queries, keys, values, cum_gate, residual, w_out, gain, w_up, w_down):
    width = HEADS * HEAD_DIM
    q_block = math.gcd(SEQUENCE_TOKENS, 512)
    key_heads = keys.astype(jnp.float32).reshape(SEQUENCE_TOKENS, HEADS, HEAD_DIM)
    value_heads = values.astype(jnp.float32).reshape(SEQUENCE_TOKENS, HEADS, HEAD_DIM)
    key_pos = jnp.arange(SEQUENCE_TOKENS, dtype=jnp.int32)
    gate_rows = cum_gate.T

    def attend(block_index):
        offset = (block_index * q_block).astype(jnp.int32)
        query_blk = lax.dynamic_slice_in_dim(queries, offset, q_block, 0).astype(jnp.float32)
        query_blk = query_blk.reshape(q_block, HEADS, HEAD_DIM)
        gate_blk = lax.dynamic_slice_in_dim(cum_gate, offset, q_block, 0)
        scores = jnp.einsum('qhd,khd->qhk', query_blk, key_heads) * HEAD_DIM ** (-0.5)
        scores = scores + gate_blk[:, :, None] - gate_rows[None, :, :]
        query_pos = offset + jnp.arange(q_block, dtype=jnp.int32)
        scores = jnp.where(key_pos[None, None, :] <= query_pos[:, None, None], scores, -1e+30)
        top = lax.optimization_barrier(jnp.max(scores, axis=-1, keepdims=True))
        weights = jnp.exp(scores - top)
        denom = lax.optimization_barrier(jnp.sum(weights, axis=-1))
        rounded = lax.optimization_barrier(weights.astype(jnp.bfloat16)).astype(jnp.float32)
        numer = jnp.einsum('qhk,khd->qhd', rounded, value_heads)
        return (numer / denom[:, :, None]).reshape(q_block, width).astype(jnp.bfloat16)
    blocks = lax.map(attend, jnp.arange(SEQUENCE_TOKENS // q_block, dtype=jnp.int32))
    attended = blocks.reshape(SEQUENCE_TOKENS, width)
    residual_sum = residual.astype(jnp.float32) + jnp.dot(attended, w_out, preferred_element_type=jnp.float32)
    mean_square = lax.optimization_barrier(jnp.mean(residual_sum * residual_sum, axis=-1, keepdims=True))
    normed = (residual_sum * lax.rsqrt(mean_square + 1e-06) * gain).astype(jnp.bfloat16)
    up_proj = jnp.dot(normed, w_up, preferred_element_type=jnp.float32)
    hidden = jnp.square(jax.nn.relu(up_proj)).astype(jnp.bfloat16)
    group = FF // N_TP
    summed = jnp.zeros((SEQUENCE_TOKENS, D), jnp.float32)
    for index in range(N_TP):
        part_out = jnp.dot(hidden[:, index * group:(index + 1) * group], w_down[index * group:(index + 1) * group], preferred_element_type=jnp.float32).astype(jnp.bfloat16)
        summed = summed + lax.optimization_barrier(part_out).astype(jnp.float32)
    return (residual_sum + summed).astype(jnp.bfloat16)
```

```python
import functools
import math

import jax
import jax.numpy as jnp
from jax import lax
from jax.experimental import pallas as pl
from jax.experimental.pallas import tpu as pltpu
from jax.sharding import PartitionSpec as P

AXES = ("sp", "tp")
LOG2E = 1.4426950408889634


class Grid:
    def __init__(self, sp, tp):
        self.y = 1 << (int(math.log2(sp)) // 2)
        self.z = sp // self.y
        self.c = 2 if tp % 2 == 0 else 1
        self.x = tp // self.c
        self.sizes = dict(z=self.z, y=self.y, x=self.x, c=self.c)

    def shift(self, data, dim, step):
        pairs = []
        for z in range(self.z):
            for y in range(self.y):
                for x in range(self.x):
                    for c in range(self.c):
                        at = dict(z=z, y=y, x=x, c=c)
                        to = dict(at)
                        to[dim] = (to[dim] + step) % self.sizes[dim]
                        pairs.append((self.flat(**at), self.flat(**to)))
        return lax.ppermute(data, AXES, pairs)

    def flat(self, z, y, x, c):
        return ((z * self.y + y) * self.x + x) * self.c + c


def attend_kernel(meta, q_ref, kv_ref, o_ref, *, shards, tok, scale):
    piece = pl.program_id(1)
    tile = pl.program_id(2)
    rows = q_ref.shape[2]
    head = q_ref.shape[3]
    own = meta[shards + piece]
    q = q_ref[0, 0]
    gate_rows = tok // head

    def block(at, carry, masked):
        top, total, acc = carry
        idx = meta[at]
        k = kv_ref[0, idx, 0:tok, :]
        v = kv_ref[0, idx, tok:2 * tok, :]
        packed = kv_ref[0, idx, 2 * tok:, :].astype(jnp.float32)
        gates = packed[0:gate_rows] + packed[gate_rows:2 * gate_rows] + packed[2 * gate_rows:3 * gate_rows]
        gates = gates * LOG2E
        gates = jnp.concatenate([gates[i:i + 1] for i in range(gate_rows)], axis=1)
        s = lax.dot_general(q, k, (((1,), (1,)), ((), ())), preferred_element_type=jnp.float32)
        s = s * (scale * LOG2E) - gates
        if masked:
            at_row = tile * rows + lax.broadcasted_iota(jnp.int32, s.shape, 0)
            at_col = lax.broadcasted_iota(jnp.int32, s.shape, 1)
            s = jnp.where(at_col <= at_row, s, -1e30)
        new_top = jnp.maximum(top, jnp.max(s, axis=1, keepdims=True))
        keep = jnp.exp2(top - new_top)
        w = jnp.exp2(s - new_top)
        total = total * keep + jnp.sum(w, axis=1, keepdims=True)
        acc = acc * keep + jnp.dot(w.astype(jnp.bfloat16), v, preferred_element_type=jnp.float32)
        return new_top, total, acc

    carry = (
        jnp.full((rows, 1), -1e30, jnp.float32),
        jnp.zeros((rows, 1), jnp.float32),
        jnp.zeros((rows, head), jnp.float32),
    )
    carry = block(own, carry, True)
    top, total, acc = lax.fori_loop(0, own, lambda at, held: block(at, held, False), carry)
    o_ref[0, 0] = (acc / total).astype(jnp.bfloat16)


def attend(meta, q, kv, shards, scale):
    groups, pieces, tok, head = q.shape
    rows = math.gcd(tok, 256)
    kernel = functools.partial(attend_kernel, shards=shards, tok=tok, scale=scale)
    return pl.pallas_call(
        kernel,
        grid_spec=pltpu.PrefetchScalarGridSpec(
            num_scalar_prefetch=1,
            grid=(groups, pieces, tok // rows),
            in_specs=[
                pl.BlockSpec((1, 1, rows, head), lambda g, j, t, meta: (g, j, t, 0)),
                pl.BlockSpec((1,) + kv.shape[1:], lambda g, j, t, meta: (g, 0, 0, 0)),
            ],
            out_specs=pl.BlockSpec((1, 1, rows, head), lambda g, j, t, meta: (g, j, t, 0)),
        ),
        out_shape=jax.ShapeDtypeStruct(q.shape, jnp.bfloat16),
        cost_estimate=pl.CostEstimate(
            flops=2 * groups * pieces * tok * tok * shards * head,
            bytes_accessed=2 * (q.size * 2 + kv.size),
            transcendentals=groups * pieces * tok * tok * shards,
        ),
        name="attend",
    )(meta, q, kv)


def split_gates(gate):
    high = lax.reduce_precision(gate, 8, 7)
    middle = lax.reduce_precision(gate - high, 8, 7)
    low = gate - high - middle
    return [part.astype(jnp.bfloat16) for part in (high, middle, low)]


def per_device(grid, queries, keys, values, cum_gate, residual, w_out, gain, w_up, w_down):
    tok, width = queries.shape
    heads = cum_gate.shape[1]
    head = width // heads
    n_z, n_y = grid.z, grid.y
    shards = n_z * n_y
    at = lax.axis_index("sp")
    at_z = at // n_y
    at_y = lax.rem(at, n_y)
    rows, d = residual.shape

    def y_of(j):
        return lax.rem(at_y - j + n_y, n_y)

    head_major = lambda a: a.reshape(tok, heads, head).transpose(1, 0, 2)
    parts = [part.T.reshape(heads, tok // head, head) for part in split_gates(cum_gate)]
    packed_gate = jnp.concatenate(parts, axis=1)
    pad = -packed_gate.shape[1] % 16
    packed_gate = jnp.pad(packed_gate, ((0, 0), (0, pad), (0, 0)))
    kv = jnp.concatenate([head_major(keys), head_major(values), packed_gate], axis=1)
    shared = heads % n_y == 0
    all_shards = jnp.arange(shards, dtype=jnp.int32)
    if shared:
        group = heads // n_y
        everything = jnp.concatenate([kv, head_major(queries)], axis=1)
        pieces = []
        for j in range(n_y):
            to = lax.rem(at_y + j, n_y)
            mine = lax.dynamic_slice_in_dim(everything, to * group, group, 0)
            pieces.append(mine if j == 0 else grid.shift(mine, "y", j))
        kv_rows = kv.shape[1]
        q = jnp.stack([piece[:, kv_rows:] for piece in pieces], axis=1)
        plane = jnp.stack([piece[:, :kv_rows] for piece in pieces], axis=1)
        planes = [plane]
        for _ in range(n_z - 1):
            planes.append(grid.shift(planes[-1], "z", 1))
        kv_all = jnp.concatenate(planes, axis=1)
        from_z = lax.rem(at_z - all_shards // n_y + n_z, n_z)
        from_y = lax.rem(at_y - lax.rem(all_shards, n_y) + n_y, n_y)
        places = from_z * n_y + from_y
        own = at_z * n_y + lax.rem(at_y - jnp.arange(n_y, dtype=jnp.int32) + n_y, n_y)
    else:
        q = head_major(queries)[:, None]
        kv_all = lax.all_gather(kv, "sp", axis=1, tiled=False)
        places = all_shards
        own = at[None]
    meta = jnp.concatenate([places, own.astype(jnp.int32)])
    out = attend(meta, q, kv_all, shards, head ** -0.5)
    if shared:
        attended = jnp.zeros((tok, heads, head), jnp.bfloat16)
        for j in range(n_y):
            piece = out[:, j]
            piece = piece if j == 0 else grid.shift(piece, "y", -j)
            start = lax.rem(at_y + j, n_y) * group
            attended = lax.dynamic_update_slice_in_dim(attended, piece.transpose(1, 0, 2), start, 1)
    else:
        attended = out[:, 0].transpose(1, 0, 2)
    attended = attended.reshape(tok, width)

    ff_here = w_up.shape[1]
    ff = ff_here // n_y
    k_rows = w_up.shape[0]
    out_cols = w_down.shape[1]
    ups, downs = [], []
    for j in range(n_y):
        to = lax.rem(at_y + j, n_y) * ff
        up = lax.dynamic_slice_in_dim(w_up, to, ff, 1)
        down = lax.dynamic_slice_in_dim(w_down, to, ff, 0)
        ups.append([up if j == 0 else grid.shift(up, "y", j)])
        downs.append([down if j == 0 else grid.shift(down, "y", j)])
    for _ in range(n_z - 1):
        for chain in ups:
            chain.append(grid.shift(chain[-1], "z", 1))
    for _ in range(n_z - 1):
        for chain in downs:
            chain.append(grid.shift(chain[-1], "z", 1))
    up_all = jnp.zeros((d, ff), jnp.bfloat16)
    for j in range(n_y):
        for k in range(n_z):
            shard = lax.rem(at_z - k + n_z, n_z) * n_y + y_of(j)
            up_all = lax.dynamic_update_slice_in_dim(up_all, ups[j][k], shard * k_rows, 0)

    mine = lax.all_to_all(attended, "tp", split_axis=0, concat_axis=1, tiled=True)
    projected = jnp.dot(mine, w_out, preferred_element_type=jnp.float32)
    residual_sum = residual.astype(jnp.float32) + projected
    mean_square = jnp.mean(residual_sum * residual_sum, axis=-1, keepdims=True)
    normed = (residual_sum * lax.rsqrt(mean_square + 1e-06) * gain).astype(jnp.bfloat16)

    def gather(data, dim):
        return [data] + [grid.shift(data, dim, j) for j in range(1, grid.sizes[dim])]

    n_x, n_c = grid.x, grid.c
    half = d // 2
    first = jnp.concatenate(gather(normed[:, :half], "x"), axis=0)
    first = jnp.concatenate(gather(first, "y"), axis=0)
    second = jnp.concatenate(gather(normed[:, half:], "y"), axis=0)
    second = gather(second, "x")
    second = jnp.concatenate(
        [second[i][j * rows:(j + 1) * rows] for j in range(n_y) for i in range(n_x)], axis=0
    )
    normed_all = jnp.concatenate(
        gather(jnp.concatenate([first, second], axis=1), "c"), axis=0
    )

    up_proj = jnp.dot(normed_all, up_all, preferred_element_type=jnp.float32)
    hidden = jnp.square(jax.nn.relu(up_proj)).astype(jnp.bfloat16)

    def scatter(data, dim):
        total = data[0].astype(jnp.float32)
        for j in range(1, grid.sizes[dim]):
            total = total + grid.shift(data[j], dim, -j).astype(jnp.float32)
        return total

    def reduce_rows(partial):
        plane_rows = n_y * n_x * rows
        here = scatter([partial[i * plane_rows:(i + 1) * plane_rows] for i in range(n_c)], "c")
        here = here.astype(jnp.bfloat16)
        cut = partial.shape[1] // 2
        line = n_x * rows
        one = here[:, :cut]
        one = scatter([one[j * line:(j + 1) * line] for j in range(n_y)], "y").astype(jnp.bfloat16)
        one = scatter([one[i * rows:(i + 1) * rows] for i in range(n_x)], "x")
        two = here[:, cut:]
        two = scatter(
            [
                jnp.concatenate(
                    [two[j * line + i * rows:j * line + (i + 1) * rows] for j in range(n_y)], axis=0
                )
                for i in range(n_x)
            ],
            "x",
        ).astype(jnp.bfloat16)
        two = scatter([two[j * rows:(j + 1) * rows] for j in range(n_y)], "y")
        return jnp.concatenate([one, two], axis=1)

    def columns(steps):
        blocks = []
        for k in steps:
            block = jnp.zeros((ff, n_y * out_cols), jnp.bfloat16)
            for j in range(n_y):
                block = lax.dynamic_update_slice_in_dim(block, downs[j][k], y_of(j) * out_cols, 1)
            blocks.append(block)
        block = jnp.concatenate(blocks, axis=1) if len(blocks) > 1 else blocks[0]
        partial = jnp.dot(hidden, block, preferred_element_type=jnp.float32).astype(jnp.bfloat16)
        return reduce_rows(partial)

    plane_cols = n_y * out_cols
    output = jnp.zeros((rows, d), jnp.bfloat16)
    batches = [list(range(n_z - 1)), [n_z - 1]] if n_z > 1 else [[0]]
    for steps in batches:
        branch = columns(steps)
        for i, k in enumerate(steps):
            start = lax.rem(at_z - k + n_z, n_z) * plane_cols
            base = lax.dynamic_slice_in_dim(residual_sum, start, plane_cols, 1)
            done = (base + branch[:, i * plane_cols:(i + 1) * plane_cols]).astype(jnp.bfloat16)
            output = lax.dynamic_update_slice_in_dim(output, done, start, 1)
    return output


def solution(mesh):
    grid = Grid(mesh.shape["sp"], mesh.shape["tp"])
    return jax.shard_map(
        functools.partial(per_device, grid),
        mesh=mesh,
        in_specs=(
            P("sp", "tp"),
            P("sp", "tp"),
            P("sp", "tp"),
            P("sp", "tp"),
            P(("sp", "tp"), None),
            P(),
            P(),
            P("sp", "tp"),
            P("tp", "sp"),
        ),
        out_specs=P(("sp", "tp"), None),
        check_vma=False,
    )
```

```python
import functools
import math

import jax
import jax.numpy as jnp
from jax import lax
from jax.experimental import pallas as pl
from jax.experimental.pallas import tpu as pltpu
from jax.sharding import PartitionSpec as P


AXES = ("sp", "tp")
LOG2E = 1.4426950408889634


class Grid:
    def __init__(self, sp, tp):
        self.y = 1 << (int(math.log2(sp)) // 2)
        self.z = sp // self.y
        self.c = 2 if tp % 2 == 0 else 1
        self.x = tp // self.c
        self.sizes = dict(z=self.z, y=self.y, x=self.x, c=self.c)

    def shift(self, data, dim, step):
        pairs = []
        for z in range(self.z):
            for y in range(self.y):
                for x in range(self.x):
                    for c in range(self.c):
                        at = dict(z=z, y=y, x=x, c=c)
                        to = dict(at)
                        to[dim] = (to[dim] + step) % self.sizes[dim]
                        pairs.append((self.flat(**at), self.flat(**to)))
        return lax.ppermute(data, AXES, pairs)

    def flat(self, z, y, x, c):
        return ((z * self.y + y) * self.x + x) * self.c + c


def attend_kernel(meta, q_ref, kv_ref, o_ref, *, shards, tok, scale):
    piece = pl.program_id(1)
    tile = pl.program_id(2)
    rows = q_ref.shape[2]
    head = q_ref.shape[3]
    own = meta[shards + piece]
    q = q_ref[0, 0]
    gate_rows = tok // head

    def block(at, carry, masked):
        top, total, acc = carry
        idx = meta[at]
        k = kv_ref[0, idx, 0:tok, :]
        v = kv_ref[0, idx, tok:2 * tok, :]
        packed = kv_ref[0, idx, 2 * tok:, :].astype(jnp.float32)
        gates = packed[0:gate_rows] + packed[gate_rows:2 * gate_rows] + packed[2 * gate_rows:3 * gate_rows]
        gates = gates * LOG2E
        gates = jnp.concatenate([gates[i:i + 1] for i in range(gate_rows)], axis=1)
        s = lax.dot_general(q, k, (((1,), (1,)), ((), ())), preferred_element_type=jnp.float32)
        s = s * (scale * LOG2E) - gates
        if masked:
            at_row = tile * rows + lax.broadcasted_iota(jnp.int32, s.shape, 0)
            at_col = lax.broadcasted_iota(jnp.int32, s.shape, 1)
            s = jnp.where(at_col <= at_row, s, -1e30)
        new_top = jnp.maximum(top, jnp.max(s, axis=1, keepdims=True))
        keep = jnp.exp2(top - new_top)
        w = jnp.exp2(s - new_top)
        total = total * keep + jnp.sum(w, axis=1, keepdims=True)
        acc = acc * keep + jnp.dot(w.astype(jnp.bfloat16), v, preferred_element_type=jnp.float32)
        return new_top, total, acc

    carry = (
        jnp.full((rows, 1), -1e30, jnp.float32),
        jnp.zeros((rows, 1), jnp.float32),
        jnp.zeros((rows, head), jnp.float32),
    )
    carry = block(own, carry, True)
    _, total, acc = lax.fori_loop(0, own, lambda at, held: block(at, held, False), carry)
    o_ref[0, 0] = (acc / total).astype(jnp.bfloat16)


def attend(meta, q, kv, shards, scale):
    groups, pieces, tok, head = q.shape
    rows = math.gcd(tok, 256)
    kernel = functools.partial(attend_kernel, shards=shards, tok=tok, scale=scale)
    return pl.pallas_call(
        kernel,
        grid_spec=pltpu.PrefetchScalarGridSpec(
            num_scalar_prefetch=1,
            grid=(groups, pieces, tok // rows),
            in_specs=[
                pl.BlockSpec((1, 1, rows, head), lambda g, j, t, meta: (g, j, t, 0)),
                pl.BlockSpec((1,) + kv.shape[1:], lambda g, j, t, meta: (g, 0, 0, 0)),
            ],
            out_specs=pl.BlockSpec((1, 1, rows, head), lambda g, j, t, meta: (g, j, t, 0)),
        ),
        out_shape=jax.ShapeDtypeStruct(q.shape, jnp.bfloat16),
        cost_estimate=pl.CostEstimate(
            flops=2 * groups * pieces * tok * tok * shards * head,
            bytes_accessed=2 * (q.size * 2 + kv.size),
            transcendentals=groups * pieces * tok * tok * shards,
        ),
        name="attend",
    )(meta, q, kv)


def split_gates(gate):
    high = lax.reduce_precision(gate, 8, 7)
    middle = lax.reduce_precision(gate - high, 8, 7)
    low = gate - high - middle
    return [part.astype(jnp.bfloat16) for part in (high, middle, low)]


def up_kernel(meta, *refs, pieces, n_y, n_x, rows, blocks, step):
    lhs = refs[:2 * pieces]
    weights = refs[2 * pieces:2 * pieces + blocks]
    out = refs[2 * pieces + blocks]
    whole = refs[2 * pieces + blocks + 1]
    k_rows = weights[0].shape[0]
    for i in range(blocks):
        whole[pl.ds(pl.multiple_of(meta[i] * k_rows, k_rows), k_rows), :] = weights[i][...]
    half = lhs[0].shape[1]
    line = n_y * n_x * rows
    for i in range(pieces):
        first = lhs[2 * i][...]
        second = lhs[2 * i + 1]
        order = [second[(x * n_y + y) * rows:(x * n_y + y + 1) * rows, :] for y in range(n_y) for x in range(n_x)]
        second = jnp.concatenate(order, axis=0)
        for at in range(0, whole.shape[1], step):
            acc = jnp.dot(first, whole[:half, at:at + step], preferred_element_type=jnp.float32)
            acc = acc + jnp.dot(second, whole[half:, at:at + step], preferred_element_type=jnp.float32)
            acc = jnp.maximum(acc, 0.0)
            out[i * line:(i + 1) * line, at:at + step] = (acc * acc).astype(jnp.bfloat16)


def up_layer(meta, halves, weights, n_y, n_x, rows):
    pieces = len(halves) // 2
    ff = weights[0].shape[1]
    d = 2 * halves[0].shape[1]
    line = n_y * n_x * rows
    kernel = functools.partial(
        up_kernel, pieces=pieces, n_y=n_y, n_x=n_x, rows=rows, blocks=len(weights), step=math.gcd(ff, 512)
    )
    vmem = pl.BlockSpec(memory_space=pltpu.VMEM)
    return pl.pallas_call(
        kernel,
        in_specs=[pl.BlockSpec(memory_space=pltpu.SMEM)] + [vmem] * (len(halves) + len(weights)),
        out_specs=vmem,
        out_shape=jax.ShapeDtypeStruct((pieces * line, ff), jnp.bfloat16),
        scratch_shapes=[pltpu.VMEM((d, ff), jnp.bfloat16)],
        cost_estimate=pl.CostEstimate(
            flops=2 * pieces * line * d * ff, bytes_accessed=2 * (pieces * line + ff) * d, transcendentals=0
        ),
        name="up",
    )(meta, *halves, *weights)


def down_kernel(meta, hidden, *refs, steps, n_y, parts, pieces):
    weights = refs[:steps * n_y]
    outs = refs[steps * n_y:]
    line = hidden.shape[0] // pieces
    per = n_y // parts
    for k in range(steps):
        for j in range(n_y):
            place = meta[j]
            part = lax.div(place, per)
            slot = part * (steps * per) + k * per + lax.rem(place, per)
            w = weights[k * n_y + j][...]
            acc = jnp.dot(hidden[...], w, preferred_element_type=jnp.float32).astype(jnp.bfloat16)
            for i in range(pieces):
                outs[i][slot] = acc[i * line:(i + 1) * line]


def down_layer(meta, hidden, weights, steps, n_y, parts, pieces):
    rows, ff = hidden.shape
    cols = weights[0].shape[1]
    kernel = functools.partial(down_kernel, steps=steps, n_y=n_y, parts=parts, pieces=pieces)
    vmem = pl.BlockSpec(memory_space=pltpu.VMEM)
    shape = jax.ShapeDtypeStruct((steps * n_y, rows // pieces, cols), jnp.bfloat16)
    return pl.pallas_call(
        kernel,
        in_specs=[pl.BlockSpec(memory_space=pltpu.SMEM), vmem] + [vmem] * len(weights),
        out_specs=[vmem] * pieces,
        out_shape=[shape] * pieces,
        cost_estimate=pl.CostEstimate(
            flops=2 * rows * ff * cols * len(weights),
            bytes_accessed=2 * (rows * ff + (rows + ff) * cols * len(weights)),
            transcendentals=0,
        ),
        name="down",
    )(meta, hidden, *weights)


def pick(places, pieces):
    out = pieces[0]
    for j in range(1, len(pieces)):
        out = jnp.where(places == j, pieces[j], out)
    return out


def per_device(grid, queries, keys, values, cum_gate, residual, w_out, gain, w_up, w_down):
    tok, width = queries.shape
    heads = cum_gate.shape[1]
    head = width // heads
    n_z, n_y, n_x, n_c = grid.z, grid.y, grid.x, grid.c
    shards = n_z * n_y
    at = lax.axis_index("sp")
    at_z = at // n_y
    at_y = lax.rem(at, n_y)
    rows, d = residual.shape

    def y_of(j):
        return lax.rem(at_y - j + n_y, n_y)

    ff = w_up.shape[1] // n_y
    out_cols = w_down.shape[1]
    ups, downs = [], []
    for j in range(n_y):
        to = lax.rem(at_y + j, n_y) * ff
        up = lax.dynamic_slice_in_dim(w_up, to, ff, 1)
        down = lax.dynamic_slice_in_dim(w_down, to, ff, 0)
        ups.append([up if j == 0 else grid.shift(up, "y", j)])
        downs.append([down if j == 0 else grid.shift(down, "y", j)])
    for _ in range(1, n_z):
        for chain in ups:
            chain.append(grid.shift(chain[-1], "z", 1))
    for _ in range(1, n_z):
        for chain in downs:
            chain.append(grid.shift(chain[-1], "z", 1))

    head_major = lambda a: a.reshape(tok, heads, head).transpose(1, 0, 2)
    parts = [part.T.reshape(heads, tok // head, head) for part in split_gates(cum_gate)]
    packed_gate = jnp.concatenate(parts, axis=1)
    pad = -packed_gate.shape[1] % 16
    packed_gate = jnp.pad(packed_gate, ((0, 0), (0, pad), (0, 0)))
    kv = jnp.concatenate([head_major(keys), head_major(values), packed_gate], axis=1)
    shared = heads % n_y == 0
    all_shards = jnp.arange(shards, dtype=jnp.int32)
    if shared:
        group = heads // n_y
        everything = jnp.concatenate([kv, head_major(queries)], axis=1)
        pieces = []
        for j in range(n_y):
            to = lax.rem(at_y + j, n_y)
            mine = lax.dynamic_slice_in_dim(everything, to * group, group, 0)
            pieces.append(mine if j == 0 else grid.shift(mine, "y", j))
        kv_rows = kv.shape[1]
        q = jnp.stack([piece[:, kv_rows:] for piece in pieces], axis=1)
        plane = jnp.stack([piece[:, :kv_rows] for piece in pieces], axis=1)
        planes = [plane]
        for _ in range(1, n_z):
            planes.append(grid.shift(planes[-1], "z", 1))
        kv_all = jnp.concatenate(planes, axis=1)
        from_z = lax.rem(at_z - all_shards // n_y + n_z, n_z)
        from_y = lax.rem(at_y - lax.rem(all_shards, n_y) + n_y, n_y)
        places = from_z * n_y + from_y
        own = at_z * n_y + lax.rem(at_y - jnp.arange(n_y, dtype=jnp.int32) + n_y, n_y)
    else:
        q = head_major(queries)[:, None]
        kv_all = lax.all_gather(kv, "sp", axis=1, tiled=False)
        places = all_shards
        own = at[None]
    meta = jnp.concatenate([places, own.astype(jnp.int32)])
    out = attend(meta, q, kv_all, shards, head ** -0.5)
    if shared:
        back = []
        for j in range(n_y):
            piece = out[:, j]
            piece = piece if j == 0 else grid.shift(piece, "y", -j)
            back.append(piece)
        blocks = []
        for b in range(n_y):
            block = pick(lax.rem(b - at_y + n_y, n_y), back)
            blocks.extend(block[g] for g in range(group))
    else:
        blocks = [out[h, 0] for h in range(heads)]
    attended = jnp.concatenate(blocks, axis=1)

    mine = lax.all_to_all(attended, "tp", split_axis=0, concat_axis=1, tiled=True)
    projected = jnp.dot(mine, w_out, preferred_element_type=jnp.float32)
    residual_sum = residual.astype(jnp.float32) + projected
    mean_square = jnp.mean(residual_sum * residual_sum, axis=-1, keepdims=True)
    normed = (residual_sum * lax.rsqrt(mean_square + 1e-06) * gain).astype(jnp.bfloat16)

    def gather(data, dim):
        found = [data]
        for j in range(1, grid.sizes[dim]):
            found.append(grid.shift(data, dim, j))
        return jnp.concatenate(found, axis=0)

    half = d // 2
    first = gather(gather(normed[:, :half], "x"), "y")
    second = gather(gather(normed[:, half:], "y"), "x")
    halves = [first, second]
    for j in range(1, n_c):
        halves.append(grid.shift(first, "c", j))
        halves.append(grid.shift(second, "c", j))
    up_meta = [
        lax.rem(at_z - k + n_z, n_z) * n_y + y_of(j) for k in range(n_z) for j in range(n_y)
    ]
    up_meta = jnp.stack(up_meta).astype(jnp.int32)
    hidden = up_layer(
        up_meta, halves, [ups[j][k] for k in range(n_z) for j in range(n_y)], n_y, n_x, rows
    )

    def scatter(pieces, dim):
        total = pieces[0].astype(jnp.float32)
        for j in range(1, grid.sizes[dim]):
            total = total + grid.shift(pieces[j], dim, -j).astype(jnp.float32)
        return total

    cuts = 2 if n_y % 2 == 0 else 1
    down_meta = up_meta[:n_y] - at_z.astype(jnp.int32) * n_y

    def columns(steps):
        weights = [downs[j][k] for k in steps for j in range(n_y)]
        partial = down_layer(down_meta, hidden, weights, len(steps), n_y, cuts, n_c)
        here = scatter(partial, "c").astype(jnp.bfloat16)
        blocks = here.shape[0] // cuts
        here = here.reshape(cuts, blocks, n_y, n_x, rows, out_cols)
        one = scatter([here[0, :, j] for j in range(n_y)], "y").astype(jnp.bfloat16)
        one = scatter([one[:, i] for i in range(n_x)], "x")
        found = [one]
        if cuts == 2:
            two = scatter([here[1, :, :, i] for i in range(n_x)], "x").astype(jnp.bfloat16)
            two = scatter([two[:, j] for j in range(n_y)], "y")
            found.append(two)
        per = n_y // cuts
        return [found[y // per][k * per + y % per] for k in range(len(steps)) for y in range(n_y)]

    plane_cols = n_y * out_cols
    output = jnp.zeros((rows, d), jnp.bfloat16)
    for steps in batches_of(n_z):
        branch = columns(steps)
        for i, k in enumerate(steps):
            start = lax.rem(at_z - k + n_z, n_z) * plane_cols
            base = lax.dynamic_slice_in_dim(residual_sum, start, plane_cols, 1)
            done = base + jnp.concatenate(branch[i * n_y:(i + 1) * n_y], axis=1)
            output = lax.dynamic_update_slice_in_dim(output, done.astype(jnp.bfloat16), start, 1)
    return output


def batches_of(n_z):
    return [list(range(n_z - 2))] + [[n_z - 2], [n_z - 1]] if n_z > 2 else [[k] for k in range(n_z)]


def solution(mesh):
    grid = Grid(mesh.shape["sp"], mesh.shape["tp"])

    def body(*args):
        return per_device(grid, *args)

    return jax.shard_map(
        body,
        mesh=mesh,
        in_specs=(
            P("sp", "tp"),
            P("sp", "tp"),
            P("sp", "tp"),
            P("sp", "tp"),
            P(("sp", "tp"), None),
            P(),
            P(),
            P("sp", "tp"),
            P("tp", "sp"),
        ),
        out_specs=P(("sp", "tp"), None),
        check_vma=False,
    )
```

```python
import functools
import math

import jax
import jax.numpy as jnp
from jax import lax
from jax.experimental import pallas as pl
from jax.experimental.pallas import tpu as pltpu
from jax.sharding import PartitionSpec as P


AXES = ("sp", "tp")
LOG2E = 1.4426950408889634


class Grid:
    def __init__(self, sp, tp):
        self.y = 1 << (int(math.log2(sp)) // 2)
        self.z = sp // self.y
        self.c = 2 if tp % 2 == 0 else 1
        self.x = tp // self.c
        self.sizes = dict(z=self.z, y=self.y, x=self.x, c=self.c)

    def shift(self, data, dim, step):
        pairs = []
        for z in range(self.z):
            for y in range(self.y):
                for x in range(self.x):
                    for c in range(self.c):
                        at = dict(z=z, y=y, x=x, c=c)
                        to = dict(at)
                        to[dim] = (to[dim] + step) % self.sizes[dim]
                        pairs.append((self.flat(**at), self.flat(**to)))
        return lax.ppermute(data, AXES, pairs)

    def flat(self, z, y, x, c):
        return ((z * self.y + y) * self.x + x) * self.c + c


def attend_kernel(meta, q_ref, kv_ref, o_ref, *, shards, tok, scale):
    piece = pl.program_id(1)
    tile = pl.program_id(2)
    rows = q_ref.shape[2]
    head = q_ref.shape[3]
    own = meta[shards + piece]
    q = q_ref[0, 0]
    gate_rows = tok // head

    def block(at, carry, masked):
        top, total, acc = carry
        idx = meta[at]
        k = kv_ref[0, idx, 0:tok, :]
        v = kv_ref[0, idx, tok:2 * tok, :]
        packed = kv_ref[0, idx, 2 * tok:, :].astype(jnp.float32)
        gates = packed[0:gate_rows] + packed[gate_rows:2 * gate_rows] + packed[2 * gate_rows:3 * gate_rows]
        gates = gates * LOG2E
        gates = jnp.concatenate([gates[i:i + 1] for i in range(gate_rows)], axis=1)
        s = lax.dot_general(q, k, (((1,), (1,)), ((), ())), preferred_element_type=jnp.float32)
        s = s * (scale * LOG2E) - gates
        if masked:
            at_row = tile * rows + lax.broadcasted_iota(jnp.int32, s.shape, 0)
            at_col = lax.broadcasted_iota(jnp.int32, s.shape, 1)
            s = jnp.where(at_col <= at_row, s, -1e30)
        new_top = jnp.maximum(top, jnp.max(s, axis=1, keepdims=True))
        keep = jnp.exp2(top - new_top)
        w = jnp.exp2(s - new_top)
        total = total * keep + jnp.sum(w, axis=1, keepdims=True)
        acc = acc * keep + jnp.dot(w.astype(jnp.bfloat16), v, preferred_element_type=jnp.float32)
        return new_top, total, acc

    carry = (
        jnp.full((rows, 1), -1e30, jnp.float32),
        jnp.zeros((rows, 1), jnp.float32),
        jnp.zeros((rows, head), jnp.float32),
    )
    carry = block(own, carry, True)
    _, total, acc = lax.fori_loop(0, own, lambda at, held: block(at, held, False), carry)
    o_ref[0, 0] = (acc / total).astype(jnp.bfloat16)


def attend(meta, q, kv, shards, scale):
    groups, pieces, tok, head = q.shape
    rows = math.gcd(tok, 512)
    kernel = functools.partial(attend_kernel, shards=shards, tok=tok, scale=scale)
    return pl.pallas_call(
        kernel,
        grid_spec=pltpu.PrefetchScalarGridSpec(
            num_scalar_prefetch=1,
            grid=(groups, pieces, tok // rows),
            in_specs=[
                pl.BlockSpec((1, 1, rows, head), lambda g, j, t, meta: (g, j, t, 0)),
                pl.BlockSpec((1,) + kv.shape[1:], lambda g, j, t, meta: (g, 0, 0, 0)),
            ],
            out_specs=pl.BlockSpec((1, 1, rows, head), lambda g, j, t, meta: (g, j, t, 0)),
        ),
        out_shape=jax.ShapeDtypeStruct(q.shape, jnp.bfloat16),
        cost_estimate=pl.CostEstimate(
            flops=2 * groups * pieces * tok * tok * shards * head,
            bytes_accessed=2 * (q.size * 2 + kv.size),
            transcendentals=groups * pieces * tok * tok * shards,
        ),
        compiler_params=pltpu.CompilerParams(vmem_limit_bytes=(12 << 20) + 4 * kv.size // groups),
        name="attend",
    )(meta, q, kv)


def split_gates(gate):
    high = lax.reduce_precision(gate, 8, 7)
    middle = lax.reduce_precision(gate - high, 8, 7)
    low = gate - high - middle
    return [part.astype(jnp.bfloat16) for part in (high, middle, low)]


def up_kernel(meta, *refs, pieces, n_y, n_x, rows, blocks, step):
    lhs = refs[:2 * pieces]
    weights = refs[2 * pieces:2 * pieces + blocks]
    out = refs[2 * pieces + blocks]
    whole = refs[2 * pieces + blocks + 1]
    k_rows = weights[0].shape[0]
    for i in range(blocks):
        whole[pl.ds(pl.multiple_of(meta[i] * k_rows, k_rows), k_rows), :] = weights[i][...]
    half = lhs[0].shape[1]
    line = n_y * n_x * rows
    for i in range(pieces):
        first = lhs[2 * i][...]
        second = lhs[2 * i + 1]
        order = [second[(x * n_y + y) * rows:(x * n_y + y + 1) * rows, :] for y in range(n_y) for x in range(n_x)]
        second = jnp.concatenate(order, axis=0)
        for at in range(0, whole.shape[1], step):
            acc = jnp.dot(first, whole[:half, at:at + step], preferred_element_type=jnp.float32)
            acc = acc + jnp.dot(second, whole[half:, at:at + step], preferred_element_type=jnp.float32)
            acc = jnp.maximum(acc, 0.0)
            out[i * line:(i + 1) * line, at:at + step] = (acc * acc).astype(jnp.bfloat16)


def up_layer(meta, halves, weights, n_y, n_x, rows):
    pieces = len(halves) // 2
    ff = weights[0].shape[1]
    d = 2 * halves[0].shape[1]
    line = n_y * n_x * rows
    kernel = functools.partial(
        up_kernel, pieces=pieces, n_y=n_y, n_x=n_x, rows=rows, blocks=len(weights), step=math.gcd(ff, 512)
    )
    vmem = pl.BlockSpec(memory_space=pltpu.VMEM)
    return pl.pallas_call(
        kernel,
        in_specs=[pl.BlockSpec(memory_space=pltpu.SMEM)] + [vmem] * (len(halves) + len(weights)),
        out_specs=vmem,
        out_shape=jax.ShapeDtypeStruct((pieces * line, ff), jnp.bfloat16),
        scratch_shapes=[pltpu.VMEM((d, ff), jnp.bfloat16)],
        cost_estimate=pl.CostEstimate(
            flops=2 * pieces * line * d * ff, bytes_accessed=2 * (pieces * line + ff) * d, transcendentals=0
        ),
        compiler_params=pltpu.CompilerParams(vmem_limit_bytes=24 << 20),
        name="up",
    )(meta, *halves, *weights)


def down_kernel(meta, hidden, *refs, steps, n_y, parts, pieces):
    weights = refs[:steps * n_y]
    outs = refs[steps * n_y:]
    line = hidden.shape[0] // pieces
    per = n_y // parts
    for k in range(steps):
        for j in range(n_y):
            place = meta[j]
            part = lax.div(place, per)
            slot = part * (steps * per) + k * per + lax.rem(place, per)
            w = weights[k * n_y + j][...]
            acc = jnp.dot(hidden[...], w, preferred_element_type=jnp.float32).astype(jnp.bfloat16)
            for i in range(pieces):
                outs[i][slot] = acc[i * line:(i + 1) * line]


def down_layer(meta, hidden, weights, steps, n_y, parts, pieces):
    rows, ff = hidden.shape
    cols = weights[0].shape[1]
    kernel = functools.partial(down_kernel, steps=steps, n_y=n_y, parts=parts, pieces=pieces)
    vmem = pl.BlockSpec(memory_space=pltpu.VMEM)
    shape = jax.ShapeDtypeStruct((steps * n_y, rows // pieces, cols), jnp.bfloat16)
    return pl.pallas_call(
        kernel,
        in_specs=[pl.BlockSpec(memory_space=pltpu.SMEM), vmem] + [vmem] * len(weights),
        out_specs=[vmem] * pieces,
        out_shape=[shape] * pieces,
        cost_estimate=pl.CostEstimate(
            flops=2 * rows * ff * cols * len(weights),
            bytes_accessed=2 * (rows * ff + (rows + ff) * cols * len(weights)),
            transcendentals=0,
        ),
        compiler_params=pltpu.CompilerParams(vmem_limit_bytes=14 << 20),
        name="down",
    )(meta, hidden, *weights)


def pick(places, pieces):
    out = pieces[0]
    for j in range(1, len(pieces)):
        out = jnp.where(places == j, pieces[j], out)
    return out


def per_device(grid, queries, keys, values, cum_gate, residual, w_out, gain, w_up, w_down):
    tok, width = queries.shape
    heads = cum_gate.shape[1]
    head = width // heads
    n_z, n_y, n_x, n_c = grid.z, grid.y, grid.x, grid.c
    shards = n_z * n_y
    at = lax.axis_index("sp")
    at_z = at // n_y
    at_y = lax.rem(at, n_y)
    rows, d = residual.shape

    def y_of(j):
        return lax.rem(at_y - j + n_y, n_y)

    ff = w_up.shape[1] // n_y
    out_cols = w_down.shape[1]
    ups, downs = [], []
    for j in range(n_y):
        to = lax.rem(at_y + j, n_y) * ff
        up = lax.dynamic_slice_in_dim(w_up, to, ff, 1)
        down = lax.dynamic_slice_in_dim(w_down, to, ff, 0)
        ups.append([up if j == 0 else grid.shift(up, "y", j)])
        downs.append([down if j == 0 else grid.shift(down, "y", j)])
    for _ in range(1, n_z):
        for chain in ups:
            chain.append(grid.shift(chain[-1], "z", 1))
    for _ in range(1, n_z):
        for chain in downs:
            chain.append(grid.shift(chain[-1], "z", 1))

    head_major = lambda a: a.reshape(tok, heads, head).transpose(1, 0, 2)
    parts = [part.T.reshape(heads, tok // head, head) for part in split_gates(cum_gate)]
    packed_gate = jnp.concatenate(parts, axis=1)
    pad = -packed_gate.shape[1] % 16
    packed_gate = jnp.pad(packed_gate, ((0, 0), (0, pad), (0, 0)))
    kv = jnp.concatenate([head_major(keys), head_major(values), packed_gate], axis=1)
    shared = heads % n_y == 0
    all_shards = jnp.arange(shards, dtype=jnp.int32)
    if shared:
        group = heads // n_y
        everything = jnp.concatenate([kv, head_major(queries)], axis=1)
        pieces = []
        for j in range(n_y):
            to = lax.rem(at_y + j, n_y)
            mine = lax.dynamic_slice_in_dim(everything, to * group, group, 0)
            pieces.append(mine if j == 0 else grid.shift(mine, "y", j))
        kv_rows = kv.shape[1]
        q = jnp.stack([piece[:, kv_rows:] for piece in pieces], axis=1)
        plane = jnp.stack([piece[:, :kv_rows] for piece in pieces], axis=1)
        planes = [plane]
        for _ in range(1, n_z):
            planes.append(grid.shift(planes[-1], "z", 1))
        kv_all = jnp.concatenate(planes, axis=1)
        from_z = lax.rem(at_z - all_shards // n_y + n_z, n_z)
        from_y = lax.rem(at_y - lax.rem(all_shards, n_y) + n_y, n_y)
        places = from_z * n_y + from_y
        own = at_z * n_y + lax.rem(at_y - jnp.arange(n_y, dtype=jnp.int32) + n_y, n_y)
    else:
        q = head_major(queries)[:, None]
        kv_all = lax.all_gather(kv, "sp", axis=1, tiled=False)
        places = all_shards
        own = at[None]
    meta = jnp.concatenate([places, own.astype(jnp.int32)])
    out = attend(meta, q, kv_all, shards, head ** -0.5)
    if shared:
        back = []
        for j in range(n_y):
            piece = out[:, j]
            piece = piece if j == 0 else grid.shift(piece, "y", -j)
            back.append(piece)
        blocks = []
        for b in range(n_y):
            block = pick(lax.rem(b - at_y + n_y, n_y), back)
            blocks.extend(block[g] for g in range(group))
    else:
        blocks = [out[h, 0] for h in range(heads)]
    attended = jnp.concatenate(blocks, axis=1)

    mine = lax.all_to_all(attended, "tp", split_axis=0, concat_axis=1, tiled=True)
    projected = jnp.dot(mine, w_out, preferred_element_type=jnp.float32)
    residual_sum = residual.astype(jnp.float32) + projected
    mean_square = jnp.mean(residual_sum * residual_sum, axis=-1, keepdims=True)
    normed = (residual_sum * lax.rsqrt(mean_square + 1e-06) * gain).astype(jnp.bfloat16)

    def gather(data, dim):
        found = [data]
        for j in range(1, grid.sizes[dim]):
            found.append(grid.shift(data, dim, j))
        return jnp.concatenate(found, axis=0)

    half = d // 2
    first = gather(gather(normed[:, :half], "x"), "y")
    second = gather(gather(normed[:, half:], "y"), "x")
    halves = [first, second]
    for j in range(1, n_c):
        halves.append(grid.shift(first, "c", j))
        halves.append(grid.shift(second, "c", j))
    up_meta = [
        lax.rem(at_z - k + n_z, n_z) * n_y + y_of(j) for k in range(n_z) for j in range(n_y)
    ]
    up_meta = jnp.stack(up_meta).astype(jnp.int32)
    hidden = up_layer(
        up_meta, halves, [ups[j][k] for k in range(n_z) for j in range(n_y)], n_y, n_x, rows
    )

    def scatter(pieces, dim):
        total = pieces[0].astype(jnp.float32)
        for j in range(1, grid.sizes[dim]):
            total = total + grid.shift(pieces[j], dim, -j).astype(jnp.float32)
        return total

    cuts = 2 if n_y % 2 == 0 else 1
    down_meta = up_meta[:n_y] - at_z.astype(jnp.int32) * n_y

    def columns(steps):
        weights = [downs[j][k] for k in steps for j in range(n_y)]
        partial = down_layer(down_meta, hidden, weights, len(steps), n_y, cuts, n_c)
        here = scatter(partial, "c").astype(jnp.bfloat16)
        blocks = here.shape[0] // cuts
        here = here.reshape(cuts, blocks, n_y, n_x, rows, out_cols)
        one = scatter([here[0, :, j] for j in range(n_y)], "y").astype(jnp.bfloat16)
        one = scatter([one[:, i] for i in range(n_x)], "x")
        found = [one]
        if cuts == 2:
            two = scatter([here[1, :, :, i] for i in range(n_x)], "x").astype(jnp.bfloat16)
            two = scatter([two[:, j] for j in range(n_y)], "y")
            found.append(two)
        per = n_y // cuts
        return [found[y // per][k * per + y % per] for k in range(len(steps)) for y in range(n_y)]

    plane_cols = n_y * out_cols
    output = jnp.zeros((rows, d), jnp.bfloat16)
    for steps in batches_of(n_z):
        branch = columns(steps)
        for i, k in enumerate(steps):
            start = lax.rem(at_z - k + n_z, n_z) * plane_cols
            base = lax.dynamic_slice_in_dim(residual_sum, start, plane_cols, 1)
            done = base + jnp.concatenate(branch[i * n_y:(i + 1) * n_y], axis=1)
            output = lax.dynamic_update_slice_in_dim(output, done.astype(jnp.bfloat16), start, 1)
    return output


def batches_of(n_z):
    return [list(range(n_z - 2))] + [[n_z - 2], [n_z - 1]] if n_z > 2 else [[k] for k in range(n_z)]


def solution(mesh):
    grid = Grid(mesh.shape["sp"], mesh.shape["tp"])

    def body(*args):
        return per_device(grid, *args)

    return jax.shard_map(
        body,
        mesh=mesh,
        in_specs=(
            P("sp", "tp"),
            P("sp", "tp"),
            P("sp", "tp"),
            P("sp", "tp"),
            P(("sp", "tp"), None),
            P(),
            P(),
            P("sp", "tp"),
            P("tp", "sp"),
        ),
        out_specs=P(("sp", "tp"), None),
        check_vma=False,
    )
```

```python
import functools
import math

import jax
import jax.numpy as jnp
from jax import lax
from jax.experimental import pallas as pl
from jax.experimental.pallas import tpu as pltpu
from jax.sharding import PartitionSpec as P


AXES = ("sp", "tp")
LOG2E = 1.4426950408889634


class Grid:
    def __init__(self, sp, tp):
        self.y = 1 << (int(math.log2(sp)) // 2)
        self.z = sp // self.y
        self.c = 2 if tp % 2 == 0 else 1
        self.x = tp // self.c
        self.sizes = dict(z=self.z, y=self.y, x=self.x, c=self.c)

    def shift(self, data, dim, step, only=None):
        pairs = []
        for z in range(self.z):
            for y in range(self.y):
                for x in range(self.x):
                    for c in range(self.c):
                        at = dict(z=z, y=y, x=x, c=c)
                        if only is not None and at[dim] not in only:
                            continue
                        to = dict(at)
                        to[dim] = (to[dim] + step) % self.sizes[dim]
                        pairs.append((self.flat(**at), self.flat(**to)))
        return lax.ppermute(data, AXES, pairs)

    def flat(self, z, y, x, c):
        return ((z * self.y + y) * self.x + x) * self.c + c


def attend_kernel(meta, q_ref, kv_ref, o_ref, *, shards, tok, scale):
    piece = pl.program_id(1)
    tile = pl.program_id(2)
    rows = q_ref.shape[2]
    head = q_ref.shape[3]
    own = meta[shards + piece]
    q = q_ref[0, 0]
    gate_rows = tok // head

    def block(at, carry, masked):
        top, total, acc = carry
        idx = meta[at]
        k = kv_ref[0, idx, 0:tok, :]
        v = kv_ref[0, idx, tok:2 * tok, :]
        packed = kv_ref[0, idx, 2 * tok:, :].astype(jnp.float32)
        gates = packed[0:gate_rows] + packed[gate_rows:2 * gate_rows] + packed[2 * gate_rows:3 * gate_rows]
        gates = gates * LOG2E
        gates = jnp.concatenate([gates[i:i + 1] for i in range(gate_rows)], axis=1)
        s = lax.dot_general(q, k, (((1,), (1,)), ((), ())), preferred_element_type=jnp.float32)
        s = s * (scale * LOG2E) - gates
        if masked:
            at_row = tile * rows + lax.broadcasted_iota(jnp.int32, s.shape, 0)
            at_col = lax.broadcasted_iota(jnp.int32, s.shape, 1)
            s = jnp.where(at_col <= at_row, s, -1e30)
        new_top = jnp.maximum(top, jnp.max(s, axis=1, keepdims=True))
        keep = jnp.exp2(top - new_top)
        w = jnp.exp2(s - new_top)
        total = total * keep + jnp.sum(w, axis=1, keepdims=True)
        acc = acc * keep + jnp.dot(w.astype(jnp.bfloat16), v, preferred_element_type=jnp.float32)
        return new_top, total, acc

    carry = (
        jnp.full((rows, 1), -1e30, jnp.float32),
        jnp.zeros((rows, 1), jnp.float32),
        jnp.zeros((rows, head), jnp.float32),
    )
    carry = block(own, carry, True)
    _, total, acc = lax.fori_loop(0, own, lambda at, held: block(at, held, False), carry)
    o_ref[0, 0] = (acc / total).astype(jnp.bfloat16)


def attend(meta, q, kv, shards, scale):
    groups, pieces, tok, head = q.shape
    rows = math.gcd(tok, 512)
    kernel = functools.partial(attend_kernel, shards=shards, tok=tok, scale=scale)
    return pl.pallas_call(
        kernel,
        grid_spec=pltpu.PrefetchScalarGridSpec(
            num_scalar_prefetch=1,
            grid=(groups, pieces, tok // rows),
            in_specs=[
                pl.BlockSpec((1, 1, rows, head), lambda g, j, t, meta: (g, j, t, 0)),
                pl.BlockSpec((1,) + kv.shape[1:], lambda g, j, t, meta: (g, 0, 0, 0)),
            ],
            out_specs=pl.BlockSpec((1, 1, rows, head), lambda g, j, t, meta: (g, j, t, 0)),
        ),
        out_shape=jax.ShapeDtypeStruct(q.shape, jnp.bfloat16),
        cost_estimate=pl.CostEstimate(
            flops=2 * groups * pieces * tok * tok * shards * head,
            bytes_accessed=2 * (q.size * 2 + kv.size),
            transcendentals=groups * pieces * tok * tok * shards,
        ),
        compiler_params=pltpu.CompilerParams(vmem_limit_bytes=(12 << 20) + 4 * kv.size // groups),
        name="attend",
    )(meta, q, kv)


def partial_kernel(meta, q_ref, own_ref, extra_ref, o_ref, *, tok, scale, mine, n_y):
    piece = pl.program_id(1)
    head = q_ref.shape[3]
    gate_rows = tok // head
    q = q_ref[0, 0]

    def block(kv_ref, idx, carry, masked):
        top, total, acc = carry
        k = kv_ref[0, idx, 0:tok, :]
        v = kv_ref[0, idx, tok:2 * tok, :]
        packed = kv_ref[0, idx, 2 * tok:, :].astype(jnp.float32)
        gates = packed[0:gate_rows] + packed[gate_rows:2 * gate_rows] + packed[2 * gate_rows:3 * gate_rows]
        gates = gates * LOG2E
        gates = jnp.concatenate([gates[i:i + 1] for i in range(gate_rows)], axis=1)
        s = lax.dot_general(q, k, (((1,), (1,)), ((), ())), preferred_element_type=jnp.float32)
        s = s * (scale * LOG2E) - gates
        if masked:
            at_row = lax.broadcasted_iota(jnp.int32, s.shape, 0)
            at_col = lax.broadcasted_iota(jnp.int32, s.shape, 1)
            s = jnp.where(at_col <= at_row, s, -1e30)
        new_top = jnp.maximum(top, jnp.max(s, axis=1, keepdims=True))
        keep = jnp.exp2(top - new_top)
        w = jnp.exp2(s - new_top)
        total = total * keep + jnp.sum(w, axis=1, keepdims=True)
        acc = acc * keep + jnp.dot(w.astype(jnp.bfloat16), v, preferred_element_type=jnp.float32)
        return new_top, total, acc

    carry = (
        jnp.full((tok, 1), -1e30, jnp.float32),
        jnp.zeros((tok, 1), jnp.float32),
        jnp.zeros((tok, head), jnp.float32),
    )
    if mine:
        carry = block(own_ref, piece, carry, True)
        for j in range(1, n_y):
            idx = lax.rem(piece + j, n_y)
            earlier = meta[2 + piece * n_y + idx]
            carry = lax.fori_loop(0, earlier, lambda _, held: block(own_ref, idx, held, False), carry)
    else:
        carry = lax.fori_loop(0, meta[0], lambda at, held: block(own_ref, at, held, False), carry)
    top, total, acc = lax.fori_loop(0, meta[1], lambda at, held: block(extra_ref, at, held, False), carry)
    total = jnp.maximum(total, 1e-30)
    o_ref[0, 0, 0:tok, :] = (acc / total).astype(o_ref.dtype)
    level = jnp.broadcast_to(top + jnp.log2(total), (tok, head)).T[0:1]
    level = jnp.concatenate([level[:, i * head:(i + 1) * head] for i in range(gate_rows)], axis=0)
    high = level.astype(jnp.bfloat16)
    rest = level - high.astype(jnp.float32)
    middle = rest.astype(jnp.bfloat16)
    low = (rest - middle.astype(jnp.float32)).astype(jnp.bfloat16)
    spare = o_ref.shape[2] - tok - 3 * gate_rows
    tail = [high.astype(jnp.float32), middle.astype(jnp.float32), low.astype(jnp.float32)]
    tail.append(jnp.zeros((spare, head), jnp.float32))
    o_ref[0, 0, tok:, :] = jnp.concatenate(tail, axis=0).astype(o_ref.dtype)


def partial_attend(meta, q, own, extra, scale, mine, dtype):
    groups, n_y, tok, head = q.shape
    tail = 3 * (tok // head)
    tail += -tail % 16
    kernel = functools.partial(partial_kernel, tok=tok, scale=scale, mine=mine, n_y=n_y)
    kv_spec = pl.BlockSpec((1,) + own.shape[1:], lambda g, j, meta: (g, 0, 0, 0))
    return pl.pallas_call(
        kernel,
        grid_spec=pltpu.PrefetchScalarGridSpec(
            num_scalar_prefetch=1,
            grid=(groups, n_y),
            in_specs=[pl.BlockSpec((1, 1, tok, head), lambda g, j, meta: (g, j, 0, 0)), kv_spec, kv_spec],
            out_specs=pl.BlockSpec((1, 1, tok + tail, head), lambda g, j, meta: (g, j, 0, 0)),
        ),
        out_shape=jax.ShapeDtypeStruct((groups, n_y, tok + tail, head), dtype),
        compiler_params=pltpu.CompilerParams(vmem_limit_bytes=20 << 20),
        cost_estimate=pl.CostEstimate(
            flops=8 * groups * n_y * n_y * tok * tok * head,
            bytes_accessed=2 * (2 * q.size + own.size + extra.size),
            transcendentals=2 * groups * n_y * n_y * tok * tok,
        ),
        name="partial",
    )(meta, q, own, extra)


def merge_kernel(meta, *refs, tok, count):
    o_ref = refs[count]
    head = o_ref.shape[3]
    gate_rows = tok // head

    def level_of(ref):
        rows = ref[0, 0, tok:, :].astype(jnp.float32)
        rows = rows[0:gate_rows] + rows[gate_rows:2 * gate_rows] + rows[2 * gate_rows:3 * gate_rows]
        row = jnp.concatenate([rows[i:i + 1] for i in range(gate_rows)], axis=1)
        return jnp.broadcast_to(row, (head, tok)).T

    levels = [level_of(refs[0])]
    for i in range(1, count):
        levels.append(jnp.where(meta[i] > 0, level_of(refs[i]), -1e30))
    top = functools.reduce(jnp.maximum, levels)
    weights = [jnp.exp2(level - top) for level in levels]
    total = functools.reduce(jnp.add, weights)
    acc = weights[0] * refs[0][0, 0, 0:tok, :].astype(jnp.float32)
    for i in range(1, count):
        acc = acc + weights[i] * refs[i][0, 0, 0:tok, :].astype(jnp.float32)
    o_ref[0, 0] = (acc / total).astype(jnp.bfloat16)


def merge(meta, parts, tok):
    groups, n_y, rows, head = parts[0].shape
    spec = pl.BlockSpec((1, 1, rows, head), lambda g, j, meta: (g, j, 0, 0))
    return pl.pallas_call(
        functools.partial(merge_kernel, tok=tok, count=len(parts)),
        grid_spec=pltpu.PrefetchScalarGridSpec(
            num_scalar_prefetch=1,
            grid=(groups, n_y),
            in_specs=[spec] * len(parts),
            out_specs=pl.BlockSpec((1, 1, tok, head), lambda g, j, meta: (g, j, 0, 0)),
        ),
        out_shape=jax.ShapeDtypeStruct((groups, n_y, tok, head), jnp.bfloat16),
        compiler_params=pltpu.CompilerParams(vmem_limit_bytes=12 << 20),
        cost_estimate=pl.CostEstimate(
            flops=8 * parts[0].size * len(parts), bytes_accessed=4 * parts[0].size * len(parts), transcendentals=0
        ),
        name="merge",
    )(meta, *parts)


def split_gates(gate):
    high = lax.reduce_precision(gate, 8, 7)
    middle = lax.reduce_precision(gate - high, 8, 7)
    low = gate - high - middle
    return [part.astype(jnp.bfloat16) for part in (high, middle, low)]


def up_kernel(meta, *refs, pieces, n_y, n_x, rows, blocks, step):
    lhs = refs[:2 * pieces]
    weights = refs[2 * pieces:2 * pieces + blocks]
    out = refs[2 * pieces + blocks]
    whole = refs[2 * pieces + blocks + 1]
    k_rows = weights[0].shape[0]
    for i in range(blocks):
        whole[pl.ds(pl.multiple_of(meta[i] * k_rows, k_rows), k_rows), :] = weights[i][...]
    half = lhs[0].shape[1]
    line = n_y * n_x * rows
    for i in range(pieces):
        first = lhs[2 * i][...]
        second = lhs[2 * i + 1]
        order = [second[(x * n_y + y) * rows:(x * n_y + y + 1) * rows, :] for y in range(n_y) for x in range(n_x)]
        second = jnp.concatenate(order, axis=0)
        for at in range(0, whole.shape[1], step):
            acc = jnp.dot(first, whole[:half, at:at + step], preferred_element_type=jnp.float32)
            acc = acc + jnp.dot(second, whole[half:, at:at + step], preferred_element_type=jnp.float32)
            acc = jnp.maximum(acc, 0.0)
            out[i * line:(i + 1) * line, at:at + step] = (acc * acc).astype(jnp.bfloat16)


def up_layer(meta, halves, weights, n_y, n_x, rows):
    pieces = len(halves) // 2
    ff = weights[0].shape[1]
    d = 2 * halves[0].shape[1]
    line = n_y * n_x * rows
    kernel = functools.partial(
        up_kernel, pieces=pieces, n_y=n_y, n_x=n_x, rows=rows, blocks=len(weights), step=math.gcd(ff, 512)
    )
    vmem = pl.BlockSpec(memory_space=pltpu.VMEM)
    return pl.pallas_call(
        kernel,
        in_specs=[pl.BlockSpec(memory_space=pltpu.SMEM)] + [vmem] * (len(halves) + len(weights)),
        out_specs=vmem,
        out_shape=jax.ShapeDtypeStruct((pieces * line, ff), jnp.bfloat16),
        scratch_shapes=[pltpu.VMEM((d, ff), jnp.bfloat16)],
        cost_estimate=pl.CostEstimate(
            flops=2 * pieces * line * d * ff, bytes_accessed=2 * (pieces * line + ff) * d, transcendentals=0
        ),
        compiler_params=pltpu.CompilerParams(vmem_limit_bytes=24 << 20),
        name="up",
    )(meta, *halves, *weights)


def down_kernel(meta, hidden, *refs, steps, n_y, parts, pieces):
    weights = refs[:steps * n_y]
    outs = refs[steps * n_y:]
    line = hidden.shape[0] // pieces
    per = n_y // parts
    for k in range(steps):
        for j in range(n_y):
            place = meta[j]
            part = lax.div(place, per)
            slot = part * (steps * per) + k * per + lax.rem(place, per)
            w = weights[k * n_y + j][...]
            acc = jnp.dot(hidden[...], w, preferred_element_type=jnp.float32).astype(jnp.bfloat16)
            for i in range(pieces):
                outs[i][slot] = acc[i * line:(i + 1) * line]


def down_layer(meta, hidden, weights, steps, n_y, parts, pieces):
    rows, ff = hidden.shape
    cols = weights[0].shape[1]
    kernel = functools.partial(down_kernel, steps=steps, n_y=n_y, parts=parts, pieces=pieces)
    vmem = pl.BlockSpec(memory_space=pltpu.VMEM)
    shape = jax.ShapeDtypeStruct((steps * n_y, rows // pieces, cols), jnp.bfloat16)
    return pl.pallas_call(
        kernel,
        in_specs=[pl.BlockSpec(memory_space=pltpu.SMEM), vmem] + [vmem] * len(weights),
        out_specs=[vmem] * pieces,
        out_shape=[shape] * pieces,
        cost_estimate=pl.CostEstimate(
            flops=2 * rows * ff * cols * len(weights),
            bytes_accessed=2 * (rows * ff + (rows + ff) * cols * len(weights)),
            transcendentals=0,
        ),
        compiler_params=pltpu.CompilerParams(vmem_limit_bytes=14 << 20),
        name="down",
    )(meta, hidden, *weights)


def pick(places, pieces):
    out = pieces[0]
    for j in range(1, len(pieces)):
        out = jnp.where(places == j, pieces[j], out)
    return out


def per_device(grid, queries, keys, values, cum_gate, residual, w_out, gain, w_up, w_down):
    tok, width = queries.shape
    heads = cum_gate.shape[1]
    head = width // heads
    n_z, n_y, n_x, n_c = grid.z, grid.y, grid.x, grid.c
    shards = n_z * n_y
    at = lax.axis_index("sp")
    at_z = at // n_y
    at_y = lax.rem(at, n_y)
    rows, d = residual.shape

    def y_of(j):
        return lax.rem(at_y - j + n_y, n_y)

    ff = w_up.shape[1] // n_y
    out_cols = w_down.shape[1]
    ups, downs = [], []
    for j in range(n_y):
        to = lax.rem(at_y + j, n_y) * ff
        up = lax.dynamic_slice_in_dim(w_up, to, ff, 1)
        down = lax.dynamic_slice_in_dim(w_down, to, ff, 0)
        ups.append([up if j == 0 else grid.shift(up, "y", j)])
        downs.append([down if j == 0 else grid.shift(down, "y", j)])
    for _ in range(1, n_z):
        for chain in ups:
            chain.append(grid.shift(chain[-1], "z", 1))
    for _ in range(1, n_z):
        for chain in downs:
            chain.append(grid.shift(chain[-1], "z", 1))

    head_major = lambda a: a.reshape(tok, heads, head).transpose(1, 0, 2)
    parts = [part.T.reshape(heads, tok // head, head) for part in split_gates(cum_gate)]
    packed_gate = jnp.concatenate(parts, axis=1)
    pad = -packed_gate.shape[1] % 16
    packed_gate = jnp.pad(packed_gate, ((0, 0), (0, pad), (0, 0)))
    kv = jnp.concatenate([head_major(keys), head_major(values), packed_gate], axis=1)
    shared = heads % n_y == 0 and n_z == 4
    scale = head ** -0.5
    if shared:
        group = heads // n_y
        everything = jnp.concatenate([kv, head_major(queries)], axis=1)
        pieces = []
        for j in range(n_y):
            to = lax.rem(at_y + j, n_y)
            mine = lax.dynamic_slice_in_dim(everything, to * group, group, 0)
            pieces.append(mine if j == 0 else grid.shift(mine, "y", j))
        kv_rows = kv.shape[1]
        q = jnp.stack([piece[:, kv_rows:] for piece in pieces], axis=1)
        plane = jnp.stack([piece[:, :kv_rows] for piece in pieces], axis=1)
        first = grid.shift(plane, "z", 1, only=(0,))
        next_q = grid.shift(q, "z", -1, only=(2, 3))
        last_q = grid.shift(q, "z", -2, only=(3,))
        flag = lambda test: jnp.where(test, n_y, 0).astype(jnp.int32)
        with_first = flag(at_z == 1)
        places = [y_of(j) for j in range(n_y)]
        earlier = [(places[i] < places[j]).astype(jnp.int32) for j in range(n_y) for i in range(n_y)]
        meta0 = jnp.stack([with_first, with_first] + earlier)
        meta1 = jnp.stack([flag((at_z == 1) | (at_z == 2)), with_first])
        meta2 = jnp.stack([with_first, with_first])
        part0 = partial_attend(meta0, q, plane, first, scale, True, jnp.float32)
        part1 = partial_attend(meta1, next_q, plane, first, scale, False, jnp.bfloat16)
        part2 = partial_attend(meta2, last_q, plane, first, scale, False, jnp.bfloat16)
        near = grid.shift(part1, "z", 1, only=(1, 2))
        far = grid.shift(part2, "z", 2, only=(1,))
        out = merge(jnp.stack([with_first, flag(at_z >= 2), flag(at_z == 3)]), [part0, near, far], tok)
    else:
        q = head_major(queries)[:, None]
        kv_all = lax.all_gather(kv, "sp", axis=1, tiled=False)
        meta = jnp.concatenate([jnp.arange(shards, dtype=jnp.int32), at[None].astype(jnp.int32)])
        out = attend(meta, q, kv_all, shards, scale)
    if shared:
        back = []
        for j in range(n_y):
            piece = out[:, j]
            piece = piece if j == 0 else grid.shift(piece, "y", -j)
            back.append(piece)
        blocks = []
        for b in range(n_y):
            block = pick(lax.rem(b - at_y + n_y, n_y), back)
            blocks.extend(block[g] for g in range(group))
    else:
        blocks = [out[h, 0] for h in range(heads)]
    attended = jnp.concatenate(blocks, axis=1)

    mine = lax.all_to_all(attended, "tp", split_axis=0, concat_axis=1, tiled=True)
    projected = jnp.dot(mine, w_out, preferred_element_type=jnp.float32)
    residual_sum = residual.astype(jnp.float32) + projected
    mean_square = jnp.mean(residual_sum * residual_sum, axis=-1, keepdims=True)
    normed = (residual_sum * lax.rsqrt(mean_square + 1e-06) * gain).astype(jnp.bfloat16)

    def gather(data, dim):
        found = [data]
        for j in range(1, grid.sizes[dim]):
            found.append(grid.shift(data, dim, j))
        return jnp.concatenate(found, axis=0)

    half = d // 2
    first = gather(gather(normed[:, :half], "x"), "y")
    second = gather(gather(normed[:, half:], "y"), "x")
    halves = [first, second]
    for j in range(1, n_c):
        halves.append(grid.shift(first, "c", j))
        halves.append(grid.shift(second, "c", j))
    up_meta = [
        lax.rem(at_z - k + n_z, n_z) * n_y + y_of(j) for k in range(n_z) for j in range(n_y)
    ]
    up_meta = jnp.stack(up_meta).astype(jnp.int32)
    hidden = up_layer(
        up_meta, halves, [ups[j][k] for k in range(n_z) for j in range(n_y)], n_y, n_x, rows
    )

    def scatter(pieces, dim):
        total = pieces[0].astype(jnp.float32)
        for j in range(1, grid.sizes[dim]):
            total = total + grid.shift(pieces[j], dim, -j).astype(jnp.float32)
        return total

    cuts = 2 if n_y % 2 == 0 else 1
    down_meta = up_meta[:n_y] - at_z.astype(jnp.int32) * n_y

    def columns(steps):
        weights = [downs[j][k] for k in steps for j in range(n_y)]
        partial = down_layer(down_meta, hidden, weights, len(steps), n_y, cuts, n_c)
        here = scatter(partial, "c").astype(jnp.bfloat16)
        blocks = here.shape[0] // cuts
        here = here.reshape(cuts, blocks, n_y, n_x, rows, out_cols)
        one = scatter([here[0, :, j] for j in range(n_y)], "y").astype(jnp.bfloat16)
        one = scatter([one[:, i] for i in range(n_x)], "x")
        found = [one]
        if cuts == 2:
            two = scatter([here[1, :, :, i] for i in range(n_x)], "x").astype(jnp.bfloat16)
            two = scatter([two[:, j] for j in range(n_y)], "y")
            found.append(two)
        per = n_y // cuts
        return [found[y // per][k * per + y % per] for k in range(len(steps)) for y in range(n_y)]

    plane_cols = n_y * out_cols
    output = jnp.zeros((rows, d), jnp.bfloat16)
    for steps in batches_of(n_z):
        branch = columns(steps)
        for i, k in enumerate(steps):
            start = lax.rem(at_z - k + n_z, n_z) * plane_cols
            base = lax.dynamic_slice_in_dim(residual_sum, start, plane_cols, 1)
            done = base + jnp.concatenate(branch[i * n_y:(i + 1) * n_y], axis=1)
            output = lax.dynamic_update_slice_in_dim(output, done.astype(jnp.bfloat16), start, 1)
    return output


def batches_of(n_z):
    return [list(range(n_z - 2))] + [[n_z - 2], [n_z - 1]] if n_z > 2 else [[k] for k in range(n_z)]


def solution(mesh):
    grid = Grid(mesh.shape["sp"], mesh.shape["tp"])

    def body(*args):
        return per_device(grid, *args)

    return jax.shard_map(
        body,
        mesh=mesh,
        in_specs=(
            P("sp", "tp"),
            P("sp", "tp"),
            P("sp", "tp"),
            P("sp", "tp"),
            P(("sp", "tp"), None),
            P(),
            P(),
            P("sp", "tp"),
            P("tp", "sp"),
        ),
        out_specs=P(("sp", "tp"), None),
        check_vma=False,
    )
```

```python
import functools
import math

import jax
import jax.numpy as jnp
from jax import lax
from jax.experimental import pallas as pl
from jax.experimental.pallas import tpu as pltpu
from jax.sharding import PartitionSpec as P


AXES = ("sp", "tp")
UP_VMEM = 24 << 20
LOG2E = 1.4426950408889634


class Grid:
    def __init__(self, sp, tp):
        self.y = 1 << (int(math.log2(sp)) // 2)
        self.z = sp // self.y
        self.c = 2 if tp % 2 == 0 else 1
        self.x = tp // self.c
        self.sizes = dict(z=self.z, y=self.y, x=self.x, c=self.c)

    def shift(self, data, dim, step, only=None, also=None):
        pairs = []
        for z in range(self.z):
            for y in range(self.y):
                for x in range(self.x):
                    for c in range(self.c):
                        at = dict(z=z, y=y, x=x, c=c)
                        if only is not None and at[dim] not in only:
                            continue
                        to = dict(at)
                        to[dim] = (to[dim] + step) % self.sizes[dim]
                        if also is not None:
                            to[also[0]] = (to[also[0]] + also[1]) % self.sizes[also[0]]
                        pairs.append((self.flat(**at), self.flat(**to)))
        return lax.ppermute(data, AXES, pairs)

    def flat(self, z, y, x, c):
        return ((z * self.y + y) * self.x + x) * self.c + c


def attend_kernel(meta, q_ref, kv_ref, o_ref, *, shards, tok, scale):
    piece = pl.program_id(1)
    tile = pl.program_id(2)
    rows = q_ref.shape[2]
    head = q_ref.shape[3]
    own = meta[shards + piece]
    q = q_ref[0, 0]
    gate_rows = tok // head

    def block(at, carry, masked):
        top, total, acc = carry
        idx = meta[at]
        k = kv_ref[0, idx, 0:tok, :]
        v = kv_ref[0, idx, tok:2 * tok, :]
        packed = kv_ref[0, idx, 2 * tok:, :].astype(jnp.float32)
        gates = packed[0:gate_rows] + packed[gate_rows:2 * gate_rows] + packed[2 * gate_rows:3 * gate_rows]
        gates = gates * LOG2E
        gates = jnp.concatenate([gates[i:i + 1] for i in range(gate_rows)], axis=1)
        s = lax.dot_general(q, k, (((1,), (1,)), ((), ())), preferred_element_type=jnp.float32)
        s = s * (scale * LOG2E) - gates
        if masked:
            at_row = tile * rows + lax.broadcasted_iota(jnp.int32, s.shape, 0)
            at_col = lax.broadcasted_iota(jnp.int32, s.shape, 1)
            s = jnp.where(at_col <= at_row, s, -1e30)
        new_top = jnp.maximum(top, jnp.max(s, axis=1, keepdims=True))
        keep = jnp.exp2(top - new_top)
        w = jnp.exp2(s - new_top)
        total = total * keep + jnp.sum(w, axis=1, keepdims=True)
        acc = acc * keep + jnp.dot(w.astype(jnp.bfloat16), v, preferred_element_type=jnp.float32)
        return new_top, total, acc

    carry = (
        jnp.full((rows, 1), -1e30, jnp.float32),
        jnp.zeros((rows, 1), jnp.float32),
        jnp.zeros((rows, head), jnp.float32),
    )
    carry = block(own, carry, True)
    _, total, acc = lax.fori_loop(0, own, lambda at, held: block(at, held, False), carry)
    o_ref[0, 0] = (acc / total).astype(jnp.bfloat16)


def attend(meta, q, kv, shards, scale):
    groups, pieces, tok, head = q.shape
    rows = math.gcd(tok, 512)
    kernel = functools.partial(attend_kernel, shards=shards, tok=tok, scale=scale)
    return pl.pallas_call(
        kernel,
        grid_spec=pltpu.PrefetchScalarGridSpec(
            num_scalar_prefetch=1,
            grid=(groups, pieces, tok // rows),
            in_specs=[
                pl.BlockSpec((1, 1, rows, head), lambda g, j, t, meta: (g, j, t, 0)),
                pl.BlockSpec((1,) + kv.shape[1:], lambda g, j, t, meta: (g, 0, 0, 0)),
            ],
            out_specs=pl.BlockSpec((1, 1, rows, head), lambda g, j, t, meta: (g, j, t, 0)),
        ),
        out_shape=jax.ShapeDtypeStruct(q.shape, jnp.bfloat16),
        cost_estimate=pl.CostEstimate(
            flops=2 * groups * pieces * tok * tok * shards * head,
            bytes_accessed=2 * (q.size * 2 + kv.size),
            transcendentals=groups * pieces * tok * tok * shards,
        ),
        compiler_params=pltpu.CompilerParams(vmem_limit_bytes=(12 << 20) + 4 * kv.size // groups),
        name="attend",
    )(meta, q, kv)


def partial_kernel(meta, q_ref, own_ref, extra_ref, o_ref, *, tok, scale, mine, n_y):
    piece = pl.program_id(1)
    head = q_ref.shape[3]
    gate_rows = tok // head
    q = q_ref[0, 0]

    def block(kv_ref, idx, carry, masked):
        top, total, acc = carry
        k = kv_ref[0, idx, 0:tok, :]
        v = kv_ref[0, idx, tok:2 * tok, :]
        packed = kv_ref[0, idx, 2 * tok:, :].astype(jnp.float32)
        gates = packed[0:gate_rows] + packed[gate_rows:2 * gate_rows] + packed[2 * gate_rows:3 * gate_rows]
        gates = gates * LOG2E
        gates = jnp.concatenate([gates[i:i + 1] for i in range(gate_rows)], axis=1)
        s = lax.dot_general(q, k, (((1,), (1,)), ((), ())), preferred_element_type=jnp.float32)
        s = s * (scale * LOG2E) - gates
        if masked:
            at_row = lax.broadcasted_iota(jnp.int32, s.shape, 0)
            at_col = lax.broadcasted_iota(jnp.int32, s.shape, 1)
            s = jnp.where(at_col <= at_row, s, -1e30)
        new_top = jnp.maximum(top, jnp.max(s, axis=1, keepdims=True))
        keep = jnp.exp2(top - new_top)
        w = jnp.exp2(s - new_top)
        total = total * keep + jnp.sum(w, axis=1, keepdims=True)
        acc = acc * keep + jnp.dot(w.astype(jnp.bfloat16), v, preferred_element_type=jnp.float32)
        return new_top, total, acc

    carry = (
        jnp.full((tok, 1), -1e30, jnp.float32),
        jnp.zeros((tok, 1), jnp.float32),
        jnp.zeros((tok, head), jnp.float32),
    )
    if mine:
        carry = block(own_ref, piece, carry, True)
        for j in range(1, n_y):
            idx = lax.rem(piece + j, n_y)
            earlier = meta[2 + piece * n_y + idx]
            carry = lax.fori_loop(0, earlier, lambda _, held: block(own_ref, idx, held, False), carry)
    else:
        carry = lax.fori_loop(0, meta[0], lambda at, held: block(own_ref, at, held, False), carry)
    top, total, acc = lax.fori_loop(0, meta[1], lambda at, held: block(extra_ref, at, held, False), carry)
    total = jnp.maximum(total, 1e-30)
    o_ref[0, 0, 0:tok, :] = (acc / total).astype(o_ref.dtype)
    level = jnp.broadcast_to(top + jnp.log2(total), (tok, head)).T[0:1]
    level = jnp.concatenate([level[:, i * head:(i + 1) * head] for i in range(gate_rows)], axis=0)
    high = level.astype(jnp.bfloat16)
    rest = level - high.astype(jnp.float32)
    middle = rest.astype(jnp.bfloat16)
    low = (rest - middle.astype(jnp.float32)).astype(jnp.bfloat16)
    spare = o_ref.shape[2] - tok - 3 * gate_rows
    tail = [high.astype(jnp.float32), middle.astype(jnp.float32), low.astype(jnp.float32)]
    tail.append(jnp.zeros((spare, head), jnp.float32))
    o_ref[0, 0, tok:, :] = jnp.concatenate(tail, axis=0).astype(o_ref.dtype)


def partial_attend(meta, q, own, extra, scale, mine, dtype):
    groups, n_y, tok, head = q.shape
    tail = 3 * (tok // head)
    tail += -tail % 16
    kernel = functools.partial(partial_kernel, tok=tok, scale=scale, mine=mine, n_y=n_y)
    kv_spec = pl.BlockSpec((1,) + own.shape[1:], lambda g, j, meta: (g, 0, 0, 0))
    return pl.pallas_call(
        kernel,
        grid_spec=pltpu.PrefetchScalarGridSpec(
            num_scalar_prefetch=1,
            grid=(groups, n_y),
            in_specs=[pl.BlockSpec((1, 1, tok, head), lambda g, j, meta: (g, j, 0, 0)), kv_spec, kv_spec],
            out_specs=pl.BlockSpec((1, 1, tok + tail, head), lambda g, j, meta: (g, j, 0, 0)),
        ),
        out_shape=jax.ShapeDtypeStruct((groups, n_y, tok + tail, head), dtype),
        compiler_params=pltpu.CompilerParams(vmem_limit_bytes=20 << 20),
        cost_estimate=pl.CostEstimate(
            flops=8 * groups * n_y * n_y * tok * tok * head,
            bytes_accessed=2 * (2 * q.size + own.size + extra.size),
            transcendentals=2 * groups * n_y * n_y * tok * tok,
        ),
        name="partial",
    )(meta, q, own, extra)


def merge_kernel(meta, *refs, tok, count):
    o_ref = refs[count]
    head = o_ref.shape[3]
    gate_rows = tok // head

    def level_of(ref):
        rows = ref[0, 0, tok:, :].astype(jnp.float32)
        rows = rows[0:gate_rows] + rows[gate_rows:2 * gate_rows] + rows[2 * gate_rows:3 * gate_rows]
        row = jnp.concatenate([rows[i:i + 1] for i in range(gate_rows)], axis=1)
        return jnp.broadcast_to(row, (head, tok)).T

    levels = [level_of(refs[0])]
    for i in range(1, count):
        levels.append(jnp.where(meta[i] > 0, level_of(refs[i]), -1e30))
    top = functools.reduce(jnp.maximum, levels)
    weights = [jnp.exp2(level - top) for level in levels]
    total = functools.reduce(jnp.add, weights)
    acc = weights[0] * refs[0][0, 0, 0:tok, :].astype(jnp.float32)
    for i in range(1, count):
        acc = acc + weights[i] * refs[i][0, 0, 0:tok, :].astype(jnp.float32)
    o_ref[0, 0] = (acc / total).astype(jnp.bfloat16)


def merge(meta, parts, tok):
    groups, n_y, rows, head = parts[0].shape
    spec = pl.BlockSpec((1, 1, rows, head), lambda g, j, meta: (g, j, 0, 0))
    return pl.pallas_call(
        functools.partial(merge_kernel, tok=tok, count=len(parts)),
        grid_spec=pltpu.PrefetchScalarGridSpec(
            num_scalar_prefetch=1,
            grid=(groups, n_y),
            in_specs=[spec] * len(parts),
            out_specs=pl.BlockSpec((1, 1, tok, head), lambda g, j, meta: (g, j, 0, 0)),
        ),
        out_shape=jax.ShapeDtypeStruct((groups, n_y, tok, head), jnp.bfloat16),
        compiler_params=pltpu.CompilerParams(vmem_limit_bytes=12 << 20),
        cost_estimate=pl.CostEstimate(
            flops=8 * parts[0].size * len(parts), bytes_accessed=4 * parts[0].size * len(parts), transcendentals=0
        ),
        name="merge",
    )(meta, *parts)


def split_gates(gate):
    high = lax.reduce_precision(gate, 8, 7)
    middle = lax.reduce_precision(gate - high, 8, 7)
    low = gate - high - middle
    return [part.astype(jnp.bfloat16) for part in (high, middle, low)]


def up_kernel(meta, *refs, pieces, n_y, n_x, rows, blocks, step):
    lhs = refs[:2 * pieces]
    weights = refs[2 * pieces:2 * pieces + blocks]
    out = refs[2 * pieces + blocks]
    whole = refs[2 * pieces + blocks + 1]
    k_rows = weights[0].shape[0]
    for i in range(blocks):
        whole[pl.ds(pl.multiple_of(meta[i] * k_rows, k_rows), k_rows), :] = weights[i][...]
    half = lhs[0].shape[1]
    line = n_y * n_x * rows
    for i in range(pieces):
        first = lhs[2 * i][...]
        second = lhs[2 * i + 1]
        order = [second[(x * n_y + y) * rows:(x * n_y + y + 1) * rows, :] for y in range(n_y) for x in range(n_x)]
        second = jnp.concatenate(order, axis=0)
        for at in range(0, whole.shape[1], step):
            acc = jnp.dot(first, whole[:half, at:at + step], preferred_element_type=jnp.float32)
            acc = acc + jnp.dot(second, whole[half:, at:at + step], preferred_element_type=jnp.float32)
            acc = jnp.maximum(acc, 0.0)
            out[i * line:(i + 1) * line, at:at + step] = (acc * acc).astype(jnp.bfloat16)


def up_layer(meta, halves, weights, n_y, n_x, rows):
    pieces = len(halves) // 2
    ff = weights[0].shape[1]
    d = 2 * halves[0].shape[1]
    line = n_y * n_x * rows
    kernel = functools.partial(
        up_kernel, pieces=pieces, n_y=n_y, n_x=n_x, rows=rows, blocks=len(weights), step=math.gcd(ff, 512)
    )
    vmem = pl.BlockSpec(memory_space=pltpu.VMEM)
    return pl.pallas_call(
        kernel,
        in_specs=[pl.BlockSpec(memory_space=pltpu.SMEM)] + [vmem] * (len(halves) + len(weights)),
        out_specs=vmem,
        out_shape=jax.ShapeDtypeStruct((pieces * line, ff), jnp.bfloat16),
        scratch_shapes=[pltpu.VMEM((d, ff), jnp.bfloat16)],
        cost_estimate=pl.CostEstimate(
            flops=2 * pieces * line * d * ff, bytes_accessed=2 * (pieces * line + ff) * d, transcendentals=0
        ),
        compiler_params=pltpu.CompilerParams(vmem_limit_bytes=UP_VMEM),
        name="up",
    )(meta, *halves, *weights)


def down_kernel(hidden, *refs, blocks, pieces):
    weights = refs[:blocks]
    outs = refs[blocks:]
    line = hidden.shape[0] // pieces
    for b in range(blocks):
        acc = jnp.dot(hidden[...], weights[b][...], preferred_element_type=jnp.float32).astype(jnp.bfloat16)
        for i in range(pieces):
            outs[i][b] = acc[i * line:(i + 1) * line]


def down_layer(hidden, weights, pieces):
    rows, ff = hidden.shape
    cols = weights[0].shape[1]
    vmem = pl.BlockSpec(memory_space=pltpu.VMEM)
    shape = jax.ShapeDtypeStruct((len(weights), rows // pieces, cols), jnp.bfloat16)
    return pl.pallas_call(
        functools.partial(down_kernel, blocks=len(weights), pieces=pieces),
        in_specs=[vmem] * (1 + len(weights)),
        out_specs=[vmem] * pieces,
        out_shape=[shape] * pieces,
        compiler_params=pltpu.CompilerParams(vmem_limit_bytes=14 << 20),
        cost_estimate=pl.CostEstimate(
            flops=2 * rows * ff * cols * len(weights),
            bytes_accessed=2 * (rows * ff + (rows + ff) * cols * len(weights)),
            transcendentals=0,
        ),
        name="down",
    )(hidden, *weights)


def settle_kernel(meta, base, *refs, plan, cols):
    out = refs[-1]
    for place, found in enumerate(plan):
        at = pl.multiple_of(meta[place] * cols, cols)
        total = base[:, pl.ds(at, cols)]
        for array, block in found:
            total = total + refs[array][block].astype(jnp.float32)
        out[:, pl.ds(at, cols)] = total.astype(out.dtype)


def settle(meta, base, arrays, plan, cols, dtype):
    vmem = pl.BlockSpec(memory_space=pltpu.VMEM)
    return pl.pallas_call(
        functools.partial(settle_kernel, plan=plan, cols=cols),
        in_specs=[pl.BlockSpec(memory_space=pltpu.SMEM)] + [vmem] * (1 + len(arrays)),
        out_specs=vmem,
        out_shape=jax.ShapeDtypeStruct(base.shape, dtype),
        compiler_params=pltpu.CompilerParams(vmem_limit_bytes=10 << 20),
        cost_estimate=pl.CostEstimate(
            flops=8 * base.size, bytes_accessed=8 * base.size, transcendentals=0
        ),
        name="settle",
    )(meta, base, *arrays)


def pick(places, pieces):
    out = pieces[0]
    for j in range(1, len(pieces)):
        out = jnp.where(places == j, pieces[j], out)
    return out


def per_device(grid, queries, keys, values, cum_gate, residual, w_out, gain, w_up, w_down):
    tok, width = queries.shape
    heads = cum_gate.shape[1]
    head = width // heads
    n_z, n_y, n_x, n_c = grid.z, grid.y, grid.x, grid.c
    shards = n_z * n_y
    at = lax.axis_index("sp")
    at_z = at // n_y
    at_y = lax.rem(at, n_y)
    rows, d = residual.shape

    def y_of(j):
        return lax.rem(at_y - j + n_y, n_y)

    ff = w_up.shape[1] // n_y
    out_cols = w_down.shape[1]
    ups, downs = [], []
    down_at = up_at = at_y
    for j in range(n_y):
        down = lax.dynamic_slice_in_dim(w_down, lax.rem(down_at + j, n_y) * ff, ff, 0)
        down_at, down = lax.optimization_barrier((down_at, down))
        downs.append([down if j == 0 else grid.shift(down, "y", j)])
    for j in reversed(range(n_y)):
        up = lax.dynamic_slice_in_dim(w_up, lax.rem(up_at + j, n_y) * ff, ff, 1)
        up_at, up = lax.optimization_barrier((up_at, up))
        ups.insert(0, [up if j == 0 else grid.shift(up, "y", j)])
    for _ in range(1, n_z):
        for chain in ups:
            chain.append(grid.shift(chain[-1], "z", 1))
    for _ in range(1, n_z):
        for chain in downs:
            chain.append(grid.shift(chain[-1], "z", 1))

    head_major = lambda a: a.reshape(tok, heads, head).transpose(1, 0, 2)
    parts = [part.T.reshape(heads, tok // head, head) for part in split_gates(cum_gate)]
    packed_gate = jnp.concatenate(parts, axis=1)
    pad = -packed_gate.shape[1] % 16
    packed_gate = jnp.pad(packed_gate, ((0, 0), (0, pad), (0, 0)))
    kv = jnp.concatenate([head_major(keys), head_major(values), packed_gate], axis=1)
    shared = heads % n_y == 0 and n_z == 4
    scale = head ** -0.5
    if shared:
        group = heads // n_y
        everything = jnp.concatenate([kv, head_major(queries)], axis=1)
        pieces = []
        for j in range(n_y):
            to = lax.rem(at_y + j, n_y)
            mine = lax.dynamic_slice_in_dim(everything, to * group, group, 0)
            pieces.append(mine if j == 0 else grid.shift(mine, "y", j))
        kv_rows = kv.shape[1]
        q = jnp.stack([piece[:, kv_rows:] for piece in pieces], axis=1)
        plane = jnp.stack([piece[:, :kv_rows] for piece in pieces], axis=1)
        first = grid.shift(plane, "z", 1, only=(0,))
        next_q = grid.shift(q, "z", -1, only=(2, 3))
        last_q = grid.shift(q, "z", -2, only=(3,))
        flag = lambda test: jnp.where(test, n_y, 0).astype(jnp.int32)
        with_first = flag(at_z == 1)
        places = [y_of(j) for j in range(n_y)]
        earlier = [(places[i] < places[j]).astype(jnp.int32) for j in range(n_y) for i in range(n_y)]
        meta0 = jnp.stack([with_first, with_first] + earlier)
        meta1 = jnp.stack([flag((at_z == 1) | (at_z == 2)), with_first])
        meta2 = jnp.stack([with_first, with_first])
        part0 = partial_attend(meta0, q, plane, first, scale, True, jnp.float32)
        part1 = partial_attend(meta1, next_q, plane, first, scale, False, jnp.bfloat16)
        part2 = partial_attend(meta2, last_q, plane, first, scale, False, jnp.bfloat16)
        near = grid.shift(part1, "z", 1, only=(1, 2))
        far = grid.shift(part2, "z", 2, only=(1,))
        out = merge(jnp.stack([with_first, flag(at_z >= 2), flag(at_z == 3)]), [part0, near, far], tok)
    else:
        q = head_major(queries)[:, None]
        kv_all = lax.all_gather(kv, "sp", axis=1, tiled=False)
        meta = jnp.concatenate([jnp.arange(shards, dtype=jnp.int32), at[None].astype(jnp.int32)])
        out = attend(meta, q, kv_all, shards, scale)
    if shared:
        back = []
        for j in range(n_y):
            piece = out[:, j]
            piece = piece if j == 0 else grid.shift(piece, "y", -j)
            back.append(piece)
        blocks = []
        for b in range(n_y):
            block = pick(lax.rem(b - at_y + n_y, n_y), back)
            blocks.extend(block[g] for g in range(group))
    else:
        blocks = [out[h, 0] for h in range(heads)]
    attended = jnp.concatenate(blocks, axis=1)

    mine = lax.all_to_all(attended, "tp", split_axis=0, concat_axis=1, tiled=True)
    projected = jnp.dot(mine, w_out, preferred_element_type=jnp.float32)
    residual_sum = residual.astype(jnp.float32) + projected
    mean_square = jnp.mean(residual_sum * residual_sum, axis=-1, keepdims=True)
    normed = (residual_sum * lax.rsqrt(mean_square + 1e-06) * gain).astype(jnp.bfloat16)

    def gather(data, dim):
        found = [data]
        for j in range(1, grid.sizes[dim]):
            found.append(grid.shift(data, dim, j))
        return jnp.concatenate(found, axis=0)

    half = d // 2
    first = gather(gather(normed[:, :half], "x"), "y")
    second = gather(gather(normed[:, half:], "y"), "x")
    halves = [first, second]
    for j in range(1, n_c):
        halves.append(grid.shift(first, "c", j))
        halves.append(grid.shift(second, "c", j))
    up_meta = [
        lax.rem(at_z - k + n_z, n_z) * n_y + y_of(j) for k in range(n_z) for j in range(n_y)
    ]
    up_meta = jnp.stack(up_meta).astype(jnp.int32)
    hidden = up_layer(
        up_meta, halves, [ups[j][k] for k in range(n_z) for j in range(n_y)], n_y, n_x, rows
    )

    def scatter(pieces, dim):
        total = pieces[0].astype(jnp.float32)
        for j in range(1, grid.sizes[dim]):
            total = total + grid.shift(pieces[j], dim, -j).astype(jnp.float32)
        return total

    batches = batches_of(n_z, n_y)
    spots = [(k, r) for k in range(n_z) for r in range(n_y)]
    starts = [lax.rem(at_z - k + n_z, n_z) * n_y + y_of(r) for k, r in spots]
    start_meta = jnp.stack(starts).astype(jnp.int32)
    total = residual_sum
    held = []
    for b, blocks in enumerate(batches):
        partial = down_layer(hidden, [downs[j][k] for k, j in blocks], n_c)
        here = scatter(partial, "c")
        here = here.reshape(len(blocks), n_y, n_x, rows, out_cols)
        held.append((here[:, 0, 0], blocks, 0))
        for dy in range(n_y):
            for dx in range(n_x):
                if dy or dx:
                    piece = here[:, dy, dx].astype(jnp.bfloat16)
                    piece = grid.shift(piece, "y", -dy, also=("x", -dx))
                    held.append((piece, blocks, dy))
        if b < len(batches) - 2:
            continue
        last = b == len(batches) - 1
        if out_cols % 128 == 0:
            plan = [
                [
                    (i, at_block)
                    for i, (_, found, dy) in enumerate(held)
                    for at_block, (k, j) in enumerate(found)
                    if (k, (j - dy) % n_y) == spot
                ]
                for spot in spots
            ]
            dtype = jnp.bfloat16 if last else jnp.float32
            total = settle(start_meta, total, [h[0] for h in held], plan, out_cols, dtype)
        else:
            for piece, found, dy in held:
                for at_block, (k, j) in enumerate(found):
                    start = starts[spots.index((k, (j - dy) % n_y))] * out_cols
                    base = lax.dynamic_slice_in_dim(total, start, out_cols, 1)
                    base = base + piece[at_block].astype(jnp.float32)
                    total = lax.dynamic_update_slice_in_dim(total, base, start, 1)
        held = []
    return total.astype(jnp.bfloat16)


def batches_of(n_z, n_y):
    blocks = [(k, j) for k in range(n_z) for j in range(n_y)]
    first = max(n_z - 2, 0) * n_y
    return [batch for batch in (blocks[:first], blocks[first:-1], blocks[-1:]) if batch]


def solution(mesh):
    grid = Grid(mesh.shape["sp"], mesh.shape["tp"])

    def body(*args):
        return per_device(grid, *args)

    return jax.shard_map(
        body,
        mesh=mesh,
        in_specs=(
            P("sp", "tp"),
            P("sp", "tp"),
            P("sp", "tp"),
            P("sp", "tp"),
            P(("sp", "tp"), None),
            P(),
            P(),
            P("sp", "tp"),
            P("tp", "sp"),
        ),
        out_specs=P(("sp", "tp"), None),
        check_vma=False,
    )
```

```python
import functools
import math

import jax
import jax.numpy as jnp
from jax import lax
from jax.experimental import pallas as pl
from jax.experimental.pallas import tpu as pltpu
from jax.sharding import PartitionSpec as P


AXES = ("sp", "tp")
UP_VMEM = 24 << 20
LOG2E = 1.4426950408889634


class Grid:
    def __init__(self, sp, tp):
        self.y = 1 << (int(math.log2(sp)) // 2)
        self.z = sp // self.y
        self.c = 2 if tp % 2 == 0 else 1
        self.x = tp // self.c
        self.sizes = dict(z=self.z, y=self.y, x=self.x, c=self.c)

    def shift(self, data, dim, step, only=None, also=None):
        pairs = []
        for z in range(self.z):
            for y in range(self.y):
                for x in range(self.x):
                    for c in range(self.c):
                        at = dict(z=z, y=y, x=x, c=c)
                        if only is not None and at[dim] not in only:
                            continue
                        to = dict(at)
                        to[dim] = (to[dim] + step) % self.sizes[dim]
                        if also is not None:
                            to[also[0]] = (to[also[0]] + also[1]) % self.sizes[also[0]]
                        pairs.append((self.flat(**at), self.flat(**to)))
        return lax.ppermute(data, AXES, pairs)

    def flat(self, z, y, x, c):
        return ((z * self.y + y) * self.x + x) * self.c + c


def attend_kernel(meta, q_ref, kv_ref, o_ref, *, shards, tok, scale):
    piece = pl.program_id(1)
    tile = pl.program_id(2)
    rows = q_ref.shape[2]
    head = q_ref.shape[3]
    own = meta[shards + piece]
    q = q_ref[0, 0]
    gate_rows = tok // head

    def block(at, carry, masked):
        top, total, acc = carry
        idx = meta[at]
        k = kv_ref[0, idx, 0:tok, :]
        v = kv_ref[0, idx, tok:2 * tok, :]
        packed = kv_ref[0, idx, 2 * tok:, :].astype(jnp.float32)
        gates = packed[0:gate_rows] + packed[gate_rows:2 * gate_rows] + packed[2 * gate_rows:3 * gate_rows]
        gates = gates * LOG2E
        gates = jnp.concatenate([gates[i:i + 1] for i in range(gate_rows)], axis=1)
        s = lax.dot_general(q, k, (((1,), (1,)), ((), ())), preferred_element_type=jnp.float32)
        s = s * (scale * LOG2E) - gates
        if masked:
            at_row = tile * rows + lax.broadcasted_iota(jnp.int32, s.shape, 0)
            at_col = lax.broadcasted_iota(jnp.int32, s.shape, 1)
            s = jnp.where(at_col <= at_row, s, -1e30)
        new_top = jnp.maximum(top, jnp.max(s, axis=1, keepdims=True))
        keep = jnp.exp2(top - new_top)
        w = jnp.exp2(s - new_top)
        total = total * keep + jnp.sum(w, axis=1, keepdims=True)
        acc = acc * keep + jnp.dot(w.astype(jnp.bfloat16), v, preferred_element_type=jnp.float32)
        return new_top, total, acc

    carry = (
        jnp.full((rows, 1), -1e30, jnp.float32),
        jnp.zeros((rows, 1), jnp.float32),
        jnp.zeros((rows, head), jnp.float32),
    )
    carry = block(own, carry, True)
    _, total, acc = lax.fori_loop(0, own, lambda at, held: block(at, held, False), carry)
    o_ref[0, 0] = (acc / total).astype(jnp.bfloat16)


def attend(meta, q, kv, shards, scale):
    groups, pieces, tok, head = q.shape
    rows = math.gcd(tok, 512)
    kernel = functools.partial(attend_kernel, shards=shards, tok=tok, scale=scale)
    return pl.pallas_call(
        kernel,
        grid_spec=pltpu.PrefetchScalarGridSpec(
            num_scalar_prefetch=1,
            grid=(groups, pieces, tok // rows),
            in_specs=[
                pl.BlockSpec((1, 1, rows, head), lambda g, j, t, meta: (g, j, t, 0)),
                pl.BlockSpec((1,) + kv.shape[1:], lambda g, j, t, meta: (g, 0, 0, 0)),
            ],
            out_specs=pl.BlockSpec((1, 1, rows, head), lambda g, j, t, meta: (g, j, t, 0)),
        ),
        out_shape=jax.ShapeDtypeStruct(q.shape, jnp.bfloat16),
        cost_estimate=pl.CostEstimate(
            flops=2 * groups * pieces * tok * tok * shards * head,
            bytes_accessed=2 * (q.size * 2 + kv.size),
            transcendentals=groups * pieces * tok * tok * shards,
        ),
        compiler_params=pltpu.CompilerParams(vmem_limit_bytes=(12 << 20) + 4 * kv.size // groups),
        name="attend",
    )(meta, q, kv)


def partial_kernel(meta, q_ref, own_ref, extra_ref, o_ref, *, tok, scale, mine, n_y):
    piece = pl.program_id(1)
    head = q_ref.shape[3]
    gate_rows = tok // head
    q = q_ref[0, 0]

    def block(kv_ref, idx, carry, masked):
        top, total, acc = carry
        k = kv_ref[0, idx, 0:tok, :]
        v = kv_ref[0, idx, tok:2 * tok, :]
        packed = kv_ref[0, idx, 2 * tok:, :].astype(jnp.float32)
        gates = packed[0:gate_rows] + packed[gate_rows:2 * gate_rows] + packed[2 * gate_rows:3 * gate_rows]
        gates = gates * LOG2E
        gates = jnp.concatenate([gates[i:i + 1] for i in range(gate_rows)], axis=1)
        s = lax.dot_general(q, k, (((1,), (1,)), ((), ())), preferred_element_type=jnp.float32)
        s = s * (scale * LOG2E) - gates
        if masked:
            at_row = lax.broadcasted_iota(jnp.int32, s.shape, 0)
            at_col = lax.broadcasted_iota(jnp.int32, s.shape, 1)
            s = jnp.where(at_col <= at_row, s, -1e30)
        new_top = jnp.maximum(top, jnp.max(s, axis=1, keepdims=True))
        keep = jnp.exp2(top - new_top)
        w = jnp.exp2(s - new_top)
        total = total * keep + jnp.sum(w, axis=1, keepdims=True)
        acc = acc * keep + jnp.dot(w.astype(jnp.bfloat16), v, preferred_element_type=jnp.float32)
        return new_top, total, acc

    carry = (
        jnp.full((tok, 1), -1e30, jnp.float32),
        jnp.zeros((tok, 1), jnp.float32),
        jnp.zeros((tok, head), jnp.float32),
    )
    if mine:
        carry = block(own_ref, piece, carry, True)
        for j in range(1, n_y):
            idx = lax.rem(piece + j, n_y)
            earlier = meta[2 + piece * n_y + idx]
            carry = lax.fori_loop(0, earlier, lambda _, held: block(own_ref, idx, held, False), carry)
    else:
        carry = lax.fori_loop(0, meta[0], lambda at, held: block(own_ref, at, held, False), carry)
    top, total, acc = lax.fori_loop(0, meta[1], lambda at, held: block(extra_ref, at, held, False), carry)
    total = jnp.maximum(total, 1e-30)
    o_ref[0, 0, 0:tok, :] = (acc / total).astype(o_ref.dtype)
    level = jnp.broadcast_to(top + jnp.log2(total), (tok, head)).T[0:1]
    level = jnp.concatenate([level[:, i * head:(i + 1) * head] for i in range(gate_rows)], axis=0)
    high = level.astype(jnp.bfloat16)
    rest = level - high.astype(jnp.float32)
    middle = rest.astype(jnp.bfloat16)
    low = (rest - middle.astype(jnp.float32)).astype(jnp.bfloat16)
    spare = o_ref.shape[2] - tok - 3 * gate_rows
    tail = [high.astype(jnp.float32), middle.astype(jnp.float32), low.astype(jnp.float32)]
    tail.append(jnp.zeros((spare, head), jnp.float32))
    o_ref[0, 0, tok:, :] = jnp.concatenate(tail, axis=0).astype(o_ref.dtype)


def partial_attend(meta, q, own, extra, scale, mine, dtype):
    groups, n_y, tok, head = q.shape
    tail = 3 * (tok // head)
    tail += -tail % 16
    kernel = functools.partial(partial_kernel, tok=tok, scale=scale, mine=mine, n_y=n_y)
    kv_spec = pl.BlockSpec((1,) + own.shape[1:], lambda g, j, meta: (g, 0, 0, 0))
    return pl.pallas_call(
        kernel,
        grid_spec=pltpu.PrefetchScalarGridSpec(
            num_scalar_prefetch=1,
            grid=(groups, n_y),
            in_specs=[pl.BlockSpec((1, 1, tok, head), lambda g, j, meta: (g, j, 0, 0)), kv_spec, kv_spec],
            out_specs=pl.BlockSpec((1, 1, tok + tail, head), lambda g, j, meta: (g, j, 0, 0)),
        ),
        out_shape=jax.ShapeDtypeStruct((groups, n_y, tok + tail, head), dtype),
        compiler_params=pltpu.CompilerParams(vmem_limit_bytes=20 << 20),
        cost_estimate=pl.CostEstimate(
            flops=8 * groups * n_y * n_y * tok * tok * head,
            bytes_accessed=2 * (2 * q.size + own.size + extra.size),
            transcendentals=2 * groups * n_y * n_y * tok * tok,
        ),
        name="partial",
    )(meta, q, own, extra)


def merge_kernel(meta, *refs, tok, count):
    o_ref = refs[count]
    head = o_ref.shape[3]
    gate_rows = tok // head

    def level_of(ref):
        rows = ref[0, 0, tok:, :].astype(jnp.float32)
        rows = rows[0:gate_rows] + rows[gate_rows:2 * gate_rows] + rows[2 * gate_rows:3 * gate_rows]
        row = jnp.concatenate([rows[i:i + 1] for i in range(gate_rows)], axis=1)
        return jnp.broadcast_to(row, (head, tok)).T

    levels = [level_of(refs[0])]
    for i in range(1, count):
        levels.append(jnp.where(meta[i] > 0, level_of(refs[i]), -1e30))
    top = functools.reduce(jnp.maximum, levels)
    weights = [jnp.exp2(level - top) for level in levels]
    total = functools.reduce(jnp.add, weights)
    acc = weights[0] * refs[0][0, 0, 0:tok, :].astype(jnp.float32)
    for i in range(1, count):
        acc = acc + weights[i] * refs[i][0, 0, 0:tok, :].astype(jnp.float32)
    o_ref[0, 0] = (acc / total).astype(jnp.bfloat16)


def merge(meta, parts, tok):
    groups, n_y, rows, head = parts[0].shape
    spec = pl.BlockSpec((1, 1, rows, head), lambda g, j, meta: (g, j, 0, 0))
    return pl.pallas_call(
        functools.partial(merge_kernel, tok=tok, count=len(parts)),
        grid_spec=pltpu.PrefetchScalarGridSpec(
            num_scalar_prefetch=1,
            grid=(groups, n_y),
            in_specs=[spec] * len(parts),
            out_specs=pl.BlockSpec((1, 1, tok, head), lambda g, j, meta: (g, j, 0, 0)),
        ),
        out_shape=jax.ShapeDtypeStruct((groups, n_y, tok, head), jnp.bfloat16),
        compiler_params=pltpu.CompilerParams(vmem_limit_bytes=12 << 20),
        cost_estimate=pl.CostEstimate(
            flops=8 * parts[0].size * len(parts), bytes_accessed=4 * parts[0].size * len(parts), transcendentals=0
        ),
        name="merge",
    )(meta, *parts)


def split_gates(gate):
    high = lax.reduce_precision(gate, 8, 7)
    middle = lax.reduce_precision(gate - high, 8, 7)
    low = gate - high - middle
    return [part.astype(jnp.bfloat16) for part in (high, middle, low)]


def up_kernel(meta, *refs, pieces, n_y, n_x, rows, blocks, step):
    parts = n_y + n_x
    lhs = refs[:parts * pieces]
    weights = refs[parts * pieces:parts * pieces + blocks]
    out = refs[parts * pieces + blocks]
    whole = refs[parts * pieces + blocks + 1]
    k_rows = weights[0].shape[0]
    for i in range(blocks):
        whole[pl.ds(pl.multiple_of(meta[i] * k_rows, k_rows), k_rows), :] = weights[i][...]
    half = lhs[0].shape[1]
    line = n_y * n_x * rows
    for i in range(pieces):
        by_y = lhs[parts * i:parts * i + n_y]
        by_x = lhs[parts * i + n_y:parts * (i + 1)]
        first = jnp.concatenate([ref[...] for ref in by_y], axis=0)
        order = [by_x[x][y * rows:(y + 1) * rows, :] for y in range(n_y) for x in range(n_x)]
        second = jnp.concatenate(order, axis=0)
        for at in range(0, whole.shape[1], step):
            acc = jnp.dot(first, whole[:half, at:at + step], preferred_element_type=jnp.float32)
            acc = acc + jnp.dot(second, whole[half:, at:at + step], preferred_element_type=jnp.float32)
            acc = jnp.maximum(acc, 0.0)
            out[i * line:(i + 1) * line, at:at + step] = (acc * acc).astype(jnp.bfloat16)


def up_layer(meta, halves, weights, n_y, n_x, rows):
    pieces = len(halves) // (n_y + n_x)
    ff = weights[0].shape[1]
    d = 2 * halves[0].shape[1]
    line = n_y * n_x * rows
    kernel = functools.partial(
        up_kernel, pieces=pieces, n_y=n_y, n_x=n_x, rows=rows, blocks=len(weights), step=math.gcd(ff, 512)
    )
    vmem = pl.BlockSpec(memory_space=pltpu.VMEM)
    return pl.pallas_call(
        kernel,
        in_specs=[pl.BlockSpec(memory_space=pltpu.SMEM)] + [vmem] * (len(halves) + len(weights)),
        out_specs=vmem,
        out_shape=jax.ShapeDtypeStruct((pieces * line, ff), jnp.bfloat16),
        scratch_shapes=[pltpu.VMEM((d, ff), jnp.bfloat16)],
        compiler_params=pltpu.CompilerParams(vmem_limit_bytes=UP_VMEM),
        cost_estimate=pl.CostEstimate(
            flops=2 * pieces * line * d * ff, bytes_accessed=2 * (pieces * line + ff) * d, transcendentals=0
        ),
        name="up",
    )(meta, *halves, *weights)


def down_kernel(hidden, *refs, blocks, pieces):
    weights = refs[:blocks]
    outs = refs[blocks:]
    line = hidden.shape[0] // pieces
    for b in range(blocks):
        acc = jnp.dot(hidden[...], weights[b][...], preferred_element_type=jnp.float32).astype(jnp.bfloat16)
        for i in range(pieces):
            outs[i][b] = acc[i * line:(i + 1) * line]


def down_layer(hidden, weights, pieces):
    rows, ff = hidden.shape
    cols = weights[0].shape[1]
    vmem = pl.BlockSpec(memory_space=pltpu.VMEM)
    shape = jax.ShapeDtypeStruct((len(weights), rows // pieces, cols), jnp.bfloat16)
    return pl.pallas_call(
        functools.partial(down_kernel, blocks=len(weights), pieces=pieces),
        in_specs=[vmem] * (1 + len(weights)),
        out_specs=[vmem] * pieces,
        out_shape=[shape] * pieces,
        compiler_params=pltpu.CompilerParams(vmem_limit_bytes=14 << 20),
        cost_estimate=pl.CostEstimate(
            flops=2 * rows * ff * cols * len(weights),
            bytes_accessed=2 * (rows * ff + (rows + ff) * cols * len(weights)),
            transcendentals=0,
        ),
        name="down",
    )(hidden, *weights)


def settle_kernel(meta, base, *refs, plan, cols):
    out = refs[-1]
    for place, found in enumerate(plan):
        at = pl.multiple_of(meta[place] * cols, cols)
        total = base[:, pl.ds(at, cols)]
        for array, block in found:
            total = total + refs[array][block].astype(jnp.float32)
        out[:, pl.ds(at, cols)] = total.astype(out.dtype)


def settle(meta, base, arrays, plan, cols, dtype):
    vmem = pl.BlockSpec(memory_space=pltpu.VMEM)
    return pl.pallas_call(
        functools.partial(settle_kernel, plan=plan, cols=cols),
        in_specs=[pl.BlockSpec(memory_space=pltpu.SMEM)] + [vmem] * (1 + len(arrays)),
        out_specs=vmem,
        out_shape=jax.ShapeDtypeStruct(base.shape, dtype),
        compiler_params=pltpu.CompilerParams(vmem_limit_bytes=10 << 20),
        cost_estimate=pl.CostEstimate(
            flops=8 * base.size, bytes_accessed=8 * base.size, transcendentals=0
        ),
        name="settle",
    )(meta, base, *arrays)


def pick(places, pieces):
    out = pieces[0]
    for j in range(1, len(pieces)):
        out = jnp.where(places == j, pieces[j], out)
    return out


def per_device(grid, queries, keys, values, cum_gate, residual, w_out, gain, w_up, w_down):
    tok, width = queries.shape
    heads = cum_gate.shape[1]
    head = width // heads
    n_z, n_y, n_x, n_c = grid.z, grid.y, grid.x, grid.c
    shards = n_z * n_y
    at = lax.axis_index("sp")
    at_z = at // n_y
    at_y = lax.rem(at, n_y)
    rows, d = residual.shape

    def y_of(j):
        return lax.rem(at_y - j + n_y, n_y)

    ff = w_up.shape[1] // n_y
    out_cols = w_down.shape[1]
    ups, downs = [], []
    down_at = up_at = at_y
    for j in range(n_y):
        down = lax.dynamic_slice_in_dim(w_down, lax.rem(down_at + j, n_y) * ff, ff, 0)
        down_at, down = lax.optimization_barrier((down_at, down))
        downs.append([down if j == 0 else grid.shift(down, "y", j)])
    for j in reversed(range(n_y)):
        up = lax.dynamic_slice_in_dim(w_up, lax.rem(up_at + j, n_y) * ff, ff, 1)
        up_at, up = lax.optimization_barrier((up_at, up))
        ups.insert(0, [up if j == 0 else grid.shift(up, "y", j)])
    for _ in range(1, n_z):
        for chain in ups:
            chain.append(grid.shift(chain[-1], "z", 1))
    for _ in range(1, n_z):
        for chain in downs:
            chain.append(grid.shift(chain[-1], "z", 1))

    head_major = lambda a: a.reshape(tok, heads, head).transpose(1, 0, 2)
    parts = [part.T.reshape(heads, tok // head, head) for part in split_gates(cum_gate)]
    packed_gate = jnp.concatenate(parts, axis=1)
    pad = -packed_gate.shape[1] % 16
    packed_gate = jnp.pad(packed_gate, ((0, 0), (0, pad), (0, 0)))
    kv = jnp.concatenate([head_major(keys), head_major(values), packed_gate], axis=1)
    shared = heads % n_y == 0 and n_z == 4
    scale = head ** -0.5
    if shared:
        group = heads // n_y
        everything = jnp.concatenate([kv, head_major(queries)], axis=1)
        pieces = []
        for j in range(n_y):
            to = lax.rem(at_y + j, n_y)
            mine = lax.dynamic_slice_in_dim(everything, to * group, group, 0)
            pieces.append(mine if j == 0 else grid.shift(mine, "y", j))
        kv_rows = kv.shape[1]
        q = jnp.stack([piece[:, kv_rows:] for piece in pieces], axis=1)
        plane = jnp.stack([piece[:, :kv_rows] for piece in pieces], axis=1)
        first = grid.shift(plane, "z", 1, only=(0,))
        next_q = grid.shift(q, "z", -1, only=(2, 3))
        last_q = grid.shift(q, "z", -2, only=(3,))
        flag = lambda test: jnp.where(test, n_y, 0).astype(jnp.int32)
        with_first = flag(at_z == 1)
        places = [y_of(j) for j in range(n_y)]
        earlier = [(places[i] < places[j]).astype(jnp.int32) for j in range(n_y) for i in range(n_y)]
        meta0 = jnp.stack([with_first, with_first] + earlier)
        meta1 = jnp.stack([flag((at_z == 1) | (at_z == 2)), with_first])
        meta2 = jnp.stack([with_first, with_first])
        part0 = partial_attend(meta0, q, plane, first, scale, True, jnp.float32)
        part1 = partial_attend(meta1, next_q, plane, first, scale, False, jnp.bfloat16)
        part2 = partial_attend(meta2, last_q, plane, first, scale, False, jnp.bfloat16)
        near = grid.shift(part1, "z", 1, only=(1, 2))
        far = grid.shift(part2, "z", 2, only=(1,))
        out = merge(jnp.stack([with_first, flag(at_z >= 2), flag(at_z == 3)]), [part0, near, far], tok)
    else:
        q = head_major(queries)[:, None]
        kv_all = lax.all_gather(kv, "sp", axis=1, tiled=False)
        meta = jnp.concatenate([jnp.arange(shards, dtype=jnp.int32), at[None].astype(jnp.int32)])
        out = attend(meta, q, kv_all, shards, scale)
    if shared:
        back = []
        for j in range(n_y):
            piece = out[:, j]
            piece = piece if j == 0 else grid.shift(piece, "y", -j)
            back.append(piece)
        blocks = []
        for b in range(n_y):
            block = pick(lax.rem(b - at_y + n_y, n_y), back)
            blocks.extend(block[g] for g in range(group))
    else:
        blocks = [out[h, 0] for h in range(heads)]
    attended = jnp.concatenate(blocks, axis=1)

    mine = lax.all_to_all(attended, "tp", split_axis=0, concat_axis=1, tiled=True)
    projected = jnp.dot(mine, w_out, preferred_element_type=jnp.float32)
    residual_sum = residual.astype(jnp.float32) + projected
    mean_square = jnp.mean(residual_sum * residual_sum, axis=-1, keepdims=True)
    normed = (residual_sum * lax.rsqrt(mean_square + 1e-06) * gain).astype(jnp.bfloat16)

    def gather(data, dim):
        found = [data]
        for j in range(1, grid.sizes[dim]):
            found.append(grid.shift(data, dim, j))
        return jnp.concatenate(found, axis=0)

    def each(data, dim):
        return [data] + [grid.shift(data, dim, j) for j in range(1, grid.sizes[dim])]

    half = d // 2
    parts = each(gather(normed[:, :half], "x"), "y")
    parts += each(gather(normed[:, half:], "y"), "x")
    halves = list(parts)
    for j in range(1, n_c):
        halves += [grid.shift(part, "c", j) for part in parts]
    up_meta = [
        lax.rem(at_z - k + n_z, n_z) * n_y + y_of(j) for k in range(n_z) for j in range(n_y)
    ]
    up_meta = jnp.stack(up_meta).astype(jnp.int32)
    hidden = up_layer(
        up_meta, halves, [ups[j][k] for k in range(n_z) for j in range(n_y)], n_y, n_x, rows
    )

    def scatter(pieces, dim):
        total = pieces[0].astype(jnp.float32)
        for j in range(1, grid.sizes[dim]):
            total = total + grid.shift(pieces[j], dim, -j).astype(jnp.float32)
        return total

    batches = batches_of(n_z, n_y)
    spots = [(k, r) for k in range(n_z) for r in range(n_y)]
    starts = [lax.rem(at_z - k + n_z, n_z) * n_y + y_of(r) for k, r in spots]
    start_meta = jnp.stack(starts).astype(jnp.int32)
    total = residual_sum
    held = []
    for b, blocks in enumerate(batches):
        partial = down_layer(hidden, [downs[j][k] for k, j in blocks], n_c)
        here = scatter(partial, "c")
        here = here.reshape(len(blocks), n_y, n_x, rows, out_cols)
        held.append((here[:, 0, 0], blocks, 0))
        for dy in range(n_y):
            for dx in range(n_x):
                if dy or dx:
                    piece = here[:, dy, dx].astype(jnp.bfloat16)
                    piece = grid.shift(piece, "y", -dy, also=("x", -dx))
                    held.append((piece, blocks, dy))
        if b < len(batches) - 2:
            continue
        last = b == len(batches) - 1
        if out_cols % 128 == 0:
            plan = [
                [
                    (i, at_block)
                    for i, (_, found, dy) in enumerate(held)
                    for at_block, (k, j) in enumerate(found)
                    if (k, (j - dy) % n_y) == spot
                ]
                for spot in spots
            ]
            dtype = jnp.bfloat16 if last else jnp.float32
            total = settle(start_meta, total, [h[0] for h in held], plan, out_cols, dtype)
        else:
            for piece, found, dy in held:
                for at_block, (k, j) in enumerate(found):
                    start = starts[spots.index((k, (j - dy) % n_y))] * out_cols
                    base = lax.dynamic_slice_in_dim(total, start, out_cols, 1)
                    base = base + piece[at_block].astype(jnp.float32)
                    total = lax.dynamic_update_slice_in_dim(total, base, start, 1)
        held = []
    return total.astype(jnp.bfloat16)


def batches_of(n_z, n_y):
    blocks = [(k, j) for k in range(n_z) for j in range(n_y)]
    first = max(n_z - 2, 0) * n_y
    return [batch for batch in (blocks[:first], blocks[first:-1], blocks[-1:]) if batch]


def solution(mesh):
    grid = Grid(mesh.shape["sp"], mesh.shape["tp"])

    def body(*args):
        return per_device(grid, *args)

    return jax.shard_map(
        body,
        mesh=mesh,
        in_specs=(
            P("sp", "tp"),
            P("sp", "tp"),
            P("sp", "tp"),
            P("sp", "tp"),
            P(("sp", "tp"), None),
            P(),
            P(),
            P("sp", "tp"),
            P("tp", "sp"),
        ),
        out_specs=P(("sp", "tp"), None),
        check_vma=False,
    )
```

```python
import functools
import math

import jax
import jax.numpy as jnp
from jax import lax
from jax.experimental import pallas as pl
from jax.experimental.pallas import tpu as pltpu
from jax.sharding import PartitionSpec as P


AXES = ("sp", "tp")
UP_VMEM = 24 << 20
LOG2E = 1.4426950408889634


class Grid:
    def __init__(self, sp, tp):
        self.y = 1 << (int(math.log2(sp)) // 2)
        self.z = sp // self.y
        self.c = 2 if tp % 2 == 0 else 1
        self.x = tp // self.c
        self.sizes = dict(z=self.z, y=self.y, x=self.x, c=self.c)

    def shift(self, data, dim, step, only=None, also=None):
        pairs = []
        for z in range(self.z):
            for y in range(self.y):
                for x in range(self.x):
                    for c in range(self.c):
                        at = dict(z=z, y=y, x=x, c=c)
                        if only is not None and at[dim] not in only:
                            continue
                        to = dict(at)
                        to[dim] = (to[dim] + step) % self.sizes[dim]
                        if also is not None:
                            to[also[0]] = (to[also[0]] + also[1]) % self.sizes[also[0]]
                        pairs.append((self.flat(**at), self.flat(**to)))
        return lax.ppermute(data, AXES, pairs)

    def flat(self, z, y, x, c):
        return ((z * self.y + y) * self.x + x) * self.c + c


def attend_kernel(meta, q_ref, kv_ref, o_ref, *, shards, tok, scale):
    piece = pl.program_id(1)
    tile = pl.program_id(2)
    rows = q_ref.shape[2]
    head = q_ref.shape[3]
    own = meta[shards + piece]
    q = q_ref[0, 0]
    gate_rows = tok // head

    def block(at, carry, masked):
        top, total, acc = carry
        idx = meta[at]
        k = kv_ref[0, idx, 0:tok, :]
        v = kv_ref[0, idx, tok:2 * tok, :]
        packed = kv_ref[0, idx, 2 * tok:, :].astype(jnp.float32)
        gates = packed[0:gate_rows] + packed[gate_rows:2 * gate_rows] + packed[2 * gate_rows:3 * gate_rows]
        gates = gates * LOG2E
        gates = jnp.concatenate([gates[i:i + 1] for i in range(gate_rows)], axis=1)
        s = lax.dot_general(q, k, (((1,), (1,)), ((), ())), preferred_element_type=jnp.float32)
        s = s * (scale * LOG2E) - gates
        if masked:
            at_row = tile * rows + lax.broadcasted_iota(jnp.int32, s.shape, 0)
            at_col = lax.broadcasted_iota(jnp.int32, s.shape, 1)
            s = jnp.where(at_col <= at_row, s, -1e30)
        new_top = jnp.maximum(top, jnp.max(s, axis=1, keepdims=True))
        keep = jnp.exp2(top - new_top)
        w = jnp.exp2(s - new_top)
        total = total * keep + jnp.sum(w, axis=1, keepdims=True)
        acc = acc * keep + jnp.dot(w.astype(jnp.bfloat16), v, preferred_element_type=jnp.float32)
        return new_top, total, acc

    carry = (
        jnp.full((rows, 1), -1e30, jnp.float32),
        jnp.zeros((rows, 1), jnp.float32),
        jnp.zeros((rows, head), jnp.float32),
    )
    carry = block(own, carry, True)
    _, total, acc = lax.fori_loop(0, own, lambda at, held: block(at, held, False), carry)
    o_ref[0, 0] = (acc / total).astype(jnp.bfloat16)


def attend(meta, q, kv, shards, scale):
    groups, pieces, tok, head = q.shape
    rows = math.gcd(tok, 512)
    kernel = functools.partial(attend_kernel, shards=shards, tok=tok, scale=scale)
    return pl.pallas_call(
        kernel,
        grid_spec=pltpu.PrefetchScalarGridSpec(
            num_scalar_prefetch=1,
            grid=(groups, pieces, tok // rows),
            in_specs=[
                pl.BlockSpec((1, 1, rows, head), lambda g, j, t, meta: (g, j, t, 0)),
                pl.BlockSpec((1,) + kv.shape[1:], lambda g, j, t, meta: (g, 0, 0, 0)),
            ],
            out_specs=pl.BlockSpec((1, 1, rows, head), lambda g, j, t, meta: (g, j, t, 0)),
        ),
        out_shape=jax.ShapeDtypeStruct(q.shape, jnp.bfloat16),
        cost_estimate=pl.CostEstimate(
            flops=2 * groups * pieces * tok * tok * shards * head,
            bytes_accessed=2 * (q.size * 2 + kv.size),
            transcendentals=groups * pieces * tok * tok * shards,
        ),
        compiler_params=pltpu.CompilerParams(vmem_limit_bytes=(12 << 20) + 4 * kv.size // groups),
        name="attend",
    )(meta, q, kv)


def partial_kernel(meta, q_ref, own_ref, extra_ref, o_ref, *, tok, scale, mine, n_y):
    piece = pl.program_id(1)
    head = q_ref.shape[3]
    gate_rows = tok // head
    q = q_ref[0, 0]

    def block(kv_ref, idx, carry, masked):
        top, total, acc = carry
        k = kv_ref[0, idx, 0:tok, :]
        v = kv_ref[0, idx, tok:2 * tok, :]
        packed = kv_ref[0, idx, 2 * tok:, :].astype(jnp.float32)
        gates = packed[0:gate_rows] + packed[gate_rows:2 * gate_rows] + packed[2 * gate_rows:3 * gate_rows]
        gates = gates * LOG2E
        gates = jnp.concatenate([gates[i:i + 1] for i in range(gate_rows)], axis=1)
        s = lax.dot_general(q, k, (((1,), (1,)), ((), ())), preferred_element_type=jnp.float32)
        s = s * (scale * LOG2E) - gates
        if masked:
            at_row = lax.broadcasted_iota(jnp.int32, s.shape, 0)
            at_col = lax.broadcasted_iota(jnp.int32, s.shape, 1)
            s = jnp.where(at_col <= at_row, s, -1e30)
        new_top = jnp.maximum(top, jnp.max(s, axis=1, keepdims=True))
        keep = jnp.exp2(top - new_top)
        w = jnp.exp2(s - new_top)
        total = total * keep + jnp.sum(w, axis=1, keepdims=True)
        acc = acc * keep + jnp.dot(w.astype(jnp.bfloat16), v, preferred_element_type=jnp.float32)
        return new_top, total, acc

    carry = (
        jnp.full((tok, 1), -1e30, jnp.float32),
        jnp.zeros((tok, 1), jnp.float32),
        jnp.zeros((tok, head), jnp.float32),
    )
    if mine:
        carry = block(own_ref, piece, carry, True)
        for j in range(1, n_y):
            idx = lax.rem(piece + j, n_y)
            earlier = meta[2 + piece * n_y + idx]
            carry = lax.fori_loop(0, earlier, lambda _, held: block(own_ref, idx, held, False), carry)
    else:
        carry = lax.fori_loop(0, meta[0], lambda at, held: block(own_ref, at, held, False), carry)
    top, total, acc = lax.fori_loop(0, meta[1], lambda at, held: block(extra_ref, at, held, False), carry)
    total = jnp.maximum(total, 1e-30)
    o_ref[0, 0, 0:tok, :] = (acc / total).astype(o_ref.dtype)
    level = jnp.broadcast_to(top + jnp.log2(total), (tok, head)).T[0:1]
    level = jnp.concatenate([level[:, i * head:(i + 1) * head] for i in range(gate_rows)], axis=0)
    high = level.astype(jnp.bfloat16)
    rest = level - high.astype(jnp.float32)
    middle = rest.astype(jnp.bfloat16)
    low = (rest - middle.astype(jnp.float32)).astype(jnp.bfloat16)
    spare = o_ref.shape[2] - tok - 3 * gate_rows
    tail = [high.astype(jnp.float32), middle.astype(jnp.float32), low.astype(jnp.float32)]
    tail.append(jnp.zeros((spare, head), jnp.float32))
    o_ref[0, 0, tok:, :] = jnp.concatenate(tail, axis=0).astype(o_ref.dtype)


def partial_attend(meta, q, own, extra, scale, mine, dtype):
    groups, n_y, tok, head = q.shape
    tail = 3 * (tok // head)
    tail += -tail % 16
    kernel = functools.partial(partial_kernel, tok=tok, scale=scale, mine=mine, n_y=n_y)
    kv_spec = pl.BlockSpec((1,) + own.shape[1:], lambda g, j, meta: (g, 0, 0, 0))
    return pl.pallas_call(
        kernel,
        grid_spec=pltpu.PrefetchScalarGridSpec(
            num_scalar_prefetch=1,
            grid=(groups, n_y),
            in_specs=[pl.BlockSpec((1, 1, tok, head), lambda g, j, meta: (g, j, 0, 0)), kv_spec, kv_spec],
            out_specs=pl.BlockSpec((1, 1, tok + tail, head), lambda g, j, meta: (g, j, 0, 0)),
        ),
        out_shape=jax.ShapeDtypeStruct((groups, n_y, tok + tail, head), dtype),
        compiler_params=pltpu.CompilerParams(vmem_limit_bytes=20 << 20),
        cost_estimate=pl.CostEstimate(
            flops=8 * groups * n_y * n_y * tok * tok * head,
            bytes_accessed=2 * (2 * q.size + own.size + extra.size),
            transcendentals=2 * groups * n_y * n_y * tok * tok,
        ),
        name="partial",
    )(meta, q, own, extra)


def merge_kernel(meta, *refs, tok, count):
    o_ref = refs[count]
    head = o_ref.shape[3]
    gate_rows = tok // head

    def level_of(ref):
        rows = ref[0, 0, tok:, :].astype(jnp.float32)
        rows = rows[0:gate_rows] + rows[gate_rows:2 * gate_rows] + rows[2 * gate_rows:3 * gate_rows]
        row = jnp.concatenate([rows[i:i + 1] for i in range(gate_rows)], axis=1)
        return jnp.broadcast_to(row, (head, tok)).T

    levels = [level_of(refs[0])]
    for i in range(1, count):
        levels.append(jnp.where(meta[i] > 0, level_of(refs[i]), -1e30))
    top = functools.reduce(jnp.maximum, levels)
    weights = [jnp.exp2(level - top) for level in levels]
    total = functools.reduce(jnp.add, weights)
    acc = weights[0] * refs[0][0, 0, 0:tok, :].astype(jnp.float32)
    for i in range(1, count):
        acc = acc + weights[i] * refs[i][0, 0, 0:tok, :].astype(jnp.float32)
    o_ref[0, 0] = (acc / total).astype(jnp.bfloat16)


def merge(meta, parts, tok):
    groups, n_y, rows, head = parts[0].shape
    spec = pl.BlockSpec((1, 1, rows, head), lambda g, j, meta: (g, j, 0, 0))
    return pl.pallas_call(
        functools.partial(merge_kernel, tok=tok, count=len(parts)),
        grid_spec=pltpu.PrefetchScalarGridSpec(
            num_scalar_prefetch=1,
            grid=(groups, n_y),
            in_specs=[spec] * len(parts),
            out_specs=pl.BlockSpec((1, 1, tok, head), lambda g, j, meta: (g, j, 0, 0)),
        ),
        out_shape=jax.ShapeDtypeStruct((groups, n_y, tok, head), jnp.bfloat16),
        compiler_params=pltpu.CompilerParams(vmem_limit_bytes=12 << 20),
        cost_estimate=pl.CostEstimate(
            flops=8 * parts[0].size * len(parts), bytes_accessed=4 * parts[0].size * len(parts), transcendentals=0
        ),
        name="merge",
    )(meta, *parts)


def split_gates(gate):
    high = lax.reduce_precision(gate, 8, 7)
    middle = lax.reduce_precision(gate - high, 8, 7)
    low = gate - high - middle
    return [part.astype(jnp.bfloat16) for part in (high, middle, low)]


def up_kernel(meta, *refs, pieces, n_y, n_x, rows, blocks, step):
    parts = n_y + n_x
    lhs = refs[:parts * pieces]
    weights = refs[parts * pieces:parts * pieces + blocks]
    out = refs[parts * pieces + blocks]
    whole = refs[parts * pieces + blocks + 1]
    k_rows = weights[0].shape[0]
    for i in range(blocks):
        whole[pl.ds(pl.multiple_of(meta[i] * k_rows, k_rows), k_rows), :] = weights[i][...]
    line = n_y * n_x * rows
    for i in range(pieces):
        by_y = lhs[parts * i:parts * i + n_y]
        by_x = lhs[parts * i + n_y:parts * (i + 1)]
        first = jnp.concatenate([ref[...] for ref in by_y], axis=0)
        order = [by_x[x][y * rows:(y + 1) * rows, :] for y in range(n_y) for x in range(n_x)]
        both = jnp.concatenate([first, jnp.concatenate(order, axis=0)], axis=1)
        for at in range(0, whole.shape[1], step):
            acc = jnp.dot(both, whole[:, at:at + step], preferred_element_type=jnp.float32)
            acc = jnp.maximum(acc, 0.0)
            out[i * line:(i + 1) * line, at:at + step] = (acc * acc).astype(jnp.bfloat16)


def up_layer(meta, halves, weights, n_y, n_x, rows):
    pieces = len(halves) // (n_y + n_x)
    ff = weights[0].shape[1]
    d = 2 * halves[0].shape[1]
    line = n_y * n_x * rows
    kernel = functools.partial(
        up_kernel, pieces=pieces, n_y=n_y, n_x=n_x, rows=rows, blocks=len(weights), step=math.gcd(ff, 512)
    )
    vmem = pl.BlockSpec(memory_space=pltpu.VMEM)
    return pl.pallas_call(
        kernel,
        in_specs=[pl.BlockSpec(memory_space=pltpu.SMEM)] + [vmem] * (len(halves) + len(weights)),
        out_specs=vmem,
        out_shape=jax.ShapeDtypeStruct((pieces * line, ff), jnp.bfloat16),
        scratch_shapes=[pltpu.VMEM((d, ff), jnp.bfloat16)],
        compiler_params=pltpu.CompilerParams(vmem_limit_bytes=UP_VMEM),
        cost_estimate=pl.CostEstimate(
            flops=2 * pieces * line * d * ff, bytes_accessed=2 * (pieces * line + ff) * d, transcendentals=0
        ),
        name="up",
    )(meta, *halves, *weights)


def down_kernel(hidden, *refs, blocks, pieces):
    weights = refs[:blocks]
    outs = refs[blocks:]
    line = hidden.shape[0] // pieces
    for b in range(blocks):
        acc = jnp.dot(hidden[...], weights[b][...], preferred_element_type=jnp.float32).astype(jnp.bfloat16)
        for i in range(pieces):
            outs[i][b] = acc[i * line:(i + 1) * line]


def down_layer(hidden, weights, pieces):
    rows, ff = hidden.shape
    cols = weights[0].shape[1]
    vmem = pl.BlockSpec(memory_space=pltpu.VMEM)
    shape = jax.ShapeDtypeStruct((len(weights), rows // pieces, cols), jnp.bfloat16)
    return pl.pallas_call(
        functools.partial(down_kernel, blocks=len(weights), pieces=pieces),
        in_specs=[vmem] * (1 + len(weights)),
        out_specs=[vmem] * pieces,
        out_shape=[shape] * pieces,
        compiler_params=pltpu.CompilerParams(vmem_limit_bytes=14 << 20),
        cost_estimate=pl.CostEstimate(
            flops=2 * rows * ff * cols * len(weights),
            bytes_accessed=2 * (rows * ff + (rows + ff) * cols * len(weights)),
            transcendentals=0,
        ),
        name="down",
    )(hidden, *weights)


def settle_kernel(meta, base, *refs, plan, cols):
    out = refs[-1]
    for place, found in enumerate(plan):
        at = pl.multiple_of(meta[place] * cols, cols)
        total = base[:, pl.ds(at, cols)]
        for array, block in found:
            total = total + refs[array][block].astype(jnp.float32)
        out[:, pl.ds(at, cols)] = total.astype(out.dtype)


def settle(meta, base, arrays, plan, cols, dtype):
    vmem = pl.BlockSpec(memory_space=pltpu.VMEM)
    return pl.pallas_call(
        functools.partial(settle_kernel, plan=plan, cols=cols),
        in_specs=[pl.BlockSpec(memory_space=pltpu.SMEM)] + [vmem] * (1 + len(arrays)),
        out_specs=vmem,
        out_shape=jax.ShapeDtypeStruct(base.shape, dtype),
        compiler_params=pltpu.CompilerParams(vmem_limit_bytes=10 << 20),
        cost_estimate=pl.CostEstimate(
            flops=8 * base.size, bytes_accessed=8 * base.size, transcendentals=0
        ),
        name="settle",
    )(meta, base, *arrays)


def pick(places, pieces):
    out = pieces[0]
    for j in range(1, len(pieces)):
        out = jnp.where(places == j, pieces[j], out)
    return out


def per_device(grid, queries, keys, values, cum_gate, residual, w_out, gain, w_up, w_down):
    tok, width = queries.shape
    heads = cum_gate.shape[1]
    head = width // heads
    n_z, n_y, n_x, n_c = grid.z, grid.y, grid.x, grid.c
    shards = n_z * n_y
    at = lax.axis_index("sp")
    at_z = at // n_y
    at_y = lax.rem(at, n_y)
    rows, d = residual.shape

    def y_of(j):
        return lax.rem(at_y - j + n_y, n_y)

    ff = w_up.shape[1] // n_y
    out_cols = w_down.shape[1]
    ups, downs = [], []
    down_at = up_at = at_y
    for j in range(n_y):
        down = lax.dynamic_slice_in_dim(w_down, lax.rem(down_at + j, n_y) * ff, ff, 0)
        down_at, down = lax.optimization_barrier((down_at, down))
        downs.append([down if j == 0 else grid.shift(down, "y", j)])
    for j in reversed(range(n_y)):
        up = lax.dynamic_slice_in_dim(w_up, lax.rem(up_at + j, n_y) * ff, ff, 1)
        up_at, up = lax.optimization_barrier((up_at, up))
        ups.insert(0, [up if j == 0 else grid.shift(up, "y", j)])
    for _ in range(1, n_z):
        for chain in ups:
            chain.append(grid.shift(chain[-1], "z", 1))
    for _ in range(1, n_z):
        for chain in downs:
            chain.append(grid.shift(chain[-1], "z", 1))

    head_major = lambda a: a.reshape(tok, heads, head).transpose(1, 0, 2)
    parts = [part.T.reshape(heads, tok // head, head) for part in split_gates(cum_gate)]
    packed_gate = jnp.concatenate(parts, axis=1)
    pad = -packed_gate.shape[1] % 16
    packed_gate = jnp.pad(packed_gate, ((0, 0), (0, pad), (0, 0)))
    kv = jnp.concatenate([head_major(keys), head_major(values), packed_gate], axis=1)
    shared = heads % n_y == 0 and n_z == 4
    scale = head ** -0.5
    if shared:
        group = heads // n_y
        everything = jnp.concatenate([kv, head_major(queries)], axis=1)
        pieces = []
        for j in range(n_y):
            to = lax.rem(at_y + j, n_y)
            mine = lax.dynamic_slice_in_dim(everything, to * group, group, 0)
            pieces.append(mine if j == 0 else grid.shift(mine, "y", j))
        kv_rows = kv.shape[1]
        q = jnp.stack([piece[:, kv_rows:] for piece in pieces], axis=1)
        plane = jnp.stack([piece[:, :kv_rows] for piece in pieces], axis=1)
        first = grid.shift(plane, "z", 1, only=(0,))
        next_q = grid.shift(q, "z", -1, only=(2, 3))
        last_q = grid.shift(q, "z", -2, only=(3,))
        flag = lambda test: jnp.where(test, n_y, 0).astype(jnp.int32)
        with_first = flag(at_z == 1)
        places = [y_of(j) for j in range(n_y)]
        earlier = [(places[i] < places[j]).astype(jnp.int32) for j in range(n_y) for i in range(n_y)]
        meta0 = jnp.stack([with_first, with_first] + earlier)
        meta1 = jnp.stack([flag((at_z == 1) | (at_z == 2)), with_first])
        meta2 = jnp.stack([with_first, with_first])
        part0 = partial_attend(meta0, q, plane, first, scale, True, jnp.float32)
        part1 = partial_attend(meta1, next_q, plane, first, scale, False, jnp.bfloat16)
        part2 = partial_attend(meta2, last_q, plane, first, scale, False, jnp.bfloat16)
        near = grid.shift(part1, "z", 1, only=(1, 2))
        far = grid.shift(part2, "z", 2, only=(1,))
        out = merge(jnp.stack([with_first, flag(at_z >= 2), flag(at_z == 3)]), [part0, near, far], tok)
    else:
        q = head_major(queries)[:, None]
        kv_all = lax.all_gather(kv, "sp", axis=1, tiled=False)
        meta = jnp.concatenate([jnp.arange(shards, dtype=jnp.int32), at[None].astype(jnp.int32)])
        out = attend(meta, q, kv_all, shards, scale)
    if shared:
        back = []
        for j in range(n_y):
            piece = out[:, j]
            piece = piece if j == 0 else grid.shift(piece, "y", -j)
            back.append(piece)
        blocks = []
        for b in range(n_y):
            block = pick(lax.rem(b - at_y + n_y, n_y), back)
            blocks.extend(block[g] for g in range(group))
    else:
        blocks = [out[h, 0] for h in range(heads)]
    attended = jnp.concatenate(blocks, axis=1)

    mine = lax.all_to_all(attended, "tp", split_axis=0, concat_axis=1, tiled=True)
    projected = jnp.dot(mine, w_out, preferred_element_type=jnp.float32)
    residual_sum = residual.astype(jnp.float32) + projected
    mean_square = jnp.mean(residual_sum * residual_sum, axis=-1, keepdims=True)
    normed = (residual_sum * lax.rsqrt(mean_square + 1e-06) * gain).astype(jnp.bfloat16)

    def gather(data, dim):
        found = [data]
        for j in range(1, grid.sizes[dim]):
            found.append(grid.shift(data, dim, j))
        return jnp.concatenate(found, axis=0)

    def each(data, dim):
        return [data] + [grid.shift(data, dim, j) for j in range(1, grid.sizes[dim])]

    half = d // 2
    parts = each(gather(normed[:, :half], "x"), "y")
    parts += each(gather(normed[:, half:], "y"), "x")
    halves = list(parts)
    for j in range(1, n_c):
        halves += [grid.shift(part, "c", j) for part in parts]
    up_meta = [
        lax.rem(at_z - k + n_z, n_z) * n_y + y_of(j) for k in range(n_z) for j in range(n_y)
    ]
    up_meta = jnp.stack(up_meta).astype(jnp.int32)
    hidden = up_layer(
        up_meta, halves, [ups[j][k] for k in range(n_z) for j in range(n_y)], n_y, n_x, rows
    )

    def scatter(pieces, dim):
        total = pieces[0].astype(jnp.float32)
        for j in range(1, grid.sizes[dim]):
            total = total + grid.shift(pieces[j], dim, -j).astype(jnp.float32)
        return total

    batches = batches_of(n_z, n_y)
    spots = [(k, r) for k in range(n_z) for r in range(n_y)]
    starts = [lax.rem(at_z - k + n_z, n_z) * n_y + y_of(r) for k, r in spots]
    start_meta = jnp.stack(starts).astype(jnp.int32)
    total = residual_sum
    held = []
    for b, blocks in enumerate(batches):
        partial = down_layer(hidden, [downs[j][k] for k, j in blocks], n_c)
        here = scatter(partial, "c")
        here = here.reshape(len(blocks), n_y, n_x, rows, out_cols)
        held.append((here[:, 0, 0], blocks, 0))
        for dy in range(n_y):
            for dx in range(n_x):
                if dy or dx:
                    piece = here[:, dy, dx].astype(jnp.bfloat16)
                    piece = grid.shift(piece, "y", -dy, also=("x", -dx))
                    held.append((piece, blocks, dy))
        if b < len(batches) - 2:
            continue
        last = b == len(batches) - 1
        if out_cols % 128 == 0:
            plan = [
                [
                    (i, at_block)
                    for i, (_, found, dy) in enumerate(held)
                    for at_block, (k, j) in enumerate(found)
                    if (k, (j - dy) % n_y) == spot
                ]
                for spot in spots
            ]
            dtype = jnp.bfloat16 if last else jnp.float32
            total = settle(start_meta, total, [h[0] for h in held], plan, out_cols, dtype)
        else:
            for piece, found, dy in held:
                for at_block, (k, j) in enumerate(found):
                    start = starts[spots.index((k, (j - dy) % n_y))] * out_cols
                    base = lax.dynamic_slice_in_dim(total, start, out_cols, 1)
                    base = base + piece[at_block].astype(jnp.float32)
                    total = lax.dynamic_update_slice_in_dim(total, base, start, 1)
        held = []
    return total.astype(jnp.bfloat16)


def batches_of(n_z, n_y):
    blocks = [(k, j) for k in range(n_z) for j in range(n_y)]
    first = max(n_z - 2, 0) * n_y
    return [batch for batch in (blocks[:first], blocks[first:-1], blocks[-1:]) if batch]


def solution(mesh):
    grid = Grid(mesh.shape["sp"], mesh.shape["tp"])

    def body(*args):
        return per_device(grid, *args)

    return jax.shard_map(
        body,
        mesh=mesh,
        in_specs=(
            P("sp", "tp"),
            P("sp", "tp"),
            P("sp", "tp"),
            P("sp", "tp"),
            P(("sp", "tp"), None),
            P(),
            P(),
            P("sp", "tp"),
            P("tp", "sp"),
        ),
        out_specs=P(("sp", "tp"), None),
        check_vma=False,
    )
```
